256 devices in a mesh: fs: 16 (over y, x), tp: 16 (over z, core).
Axes of the slice: x: 4, y: 4, z: 8, core: 2. Of those that a mesh axis runs over, the one named last changes fastest.
Arguments:
- tokens: bfloat16 [32768, 2048], P(('fs', 'tp')), may hold values from -6 to 6
- norm_gain: float32 [2048], replicated, may hold values from 0.1 to 1.9
- gate_weight: bfloat16 [2048, 5632], P('fs', 'tp'), may hold values from -0.125 to 0.125
- up_weight: bfloat16 [2048, 5632], P('fs', 'tp'), may hold values from -0.125 to 0.125
- down_weight: bfloat16 [5632, 2048], P('tp', 'fs'), may hold values from -0.078125 to 0.078125
Outputs:
- mixed: bfloat16 [32768, 2048], P(('fs', 'tp'))
The draws below stay inside these ranges and needn't reach their ends.
All inputs are finite; a program needn't handle non-finite values.
Results may differ from the reference program's by a relative error of at most 0.0065.
Values may be sent and summed in bfloat16 or wider, within the bound.
No kernel may reach another device: no remote copies, remote signals or barrier semaphores. Data moves between devices by JAX's collectives and lax.ppermute only.
A program may use at most 128 MiB of HBM per device.

```python
import jax
import jax.numpy as jnp
from jax import lax

D = 2048
FF = 5632
TOK_DEV = 128
TOKENS = 32768


def shard_levels(stream_key, extent, pieces, low, high):
    factor_of = 1.0
    for dim, blocks in pieces:
        draws = jax.random.uniform(jax.random.fold_in(jax.random.fold_in(stream_key, 6), dim), (blocks,), jnp.float32, low / len(pieces), high / len(pieces))
        factor_of = factor_of * jnp.repeat(jnp.exp(draws), extent[dim] // blocks).reshape((-1,) + (1,) * (len(extent) - 1 - dim))
    return factor_of


def centred(key, dims, scale, limit, cuts=(), held_as=jnp.bfloat16):
    loudness = shard_levels(key, dims, cuts, -0.22, 0.18) if cuts else 1.0
    entries = jax.random.normal(key, dims, jnp.float32) * scale * loudness
    return jnp.minimum(jnp.maximum(entries, -limit), limit).astype(held_as)


def setup_inputs(seed: int = 0) -> dict:
    streams_of = jax.random.split(jax.random.key(seed), 6)
    return {
        "tokens": centred(streams_of[0], (TOKENS, D), 1.0, 6.0, ((0, 256),)),
        "norm_gain": jnp.clip(1.0 + 0.18 * jax.random.normal(streams_of[1], (D,), jnp.float32), 0.1, 1.9),
        "gate_weight": centred(streams_of[2], (D, FF), D ** -0.5, 0.125, ((0, 16), (1, 16))),
        "up_weight": centred(streams_of[3], (D, FF), D ** -0.5, 0.125, ((0, 16), (1, 16))),
        "down_weight": centred(streams_of[4], (FF, D), FF ** -0.5, 0.078125, ((0, 16), (1, 16))),
    }


eps_floor = 0.05

def reference(tokens, norm_gain, gate_weight, up_weight, down_weight):
    blocks = tokens.reshape(-1, TOK_DEV, D)

    def one_block(rows):
        values = rows.astype(jnp.float32)
        factor = lax.rsqrt(lax.optimization_barrier(jnp.mean(values * values, axis=-1, keepdims=True)) + eps_floor)
        normed = (values * factor * norm_gain).astype(jnp.bfloat16)
        gate = jnp.dot(normed, gate_weight, preferred_element_type=jnp.float32)
        upper = jnp.dot(normed, up_weight, preferred_element_type=jnp.float32)
        hidden = (jax.nn.silu(gate) * upper).astype(jnp.bfloat16)
        return jnp.dot(hidden, down_weight, preferred_element_type=jnp.float32).astype(jnp.bfloat16)
    return lax.map(one_block, blocks).reshape(TOKENS, D)
```

```python
import jax
import jax.numpy as jnp
from jax import lax
from jax.sharding import Mesh, PartitionSpec as P

eps_floor = 0.05
Z = 8


def shift(x, by):
    return lax.ppermute(x, "z", [(i, (i + by) % Z) for i in range(Z)])


def swap(x):
    return lax.ppermute(x, "c", [(0, 1), (1, 0)])


def from_everyone(x, axis):
    length = lax.axis_size(axis)
    return lax.all_to_all(jnp.broadcast_to(x[None], (length, *x.shape)), axis, 0, 0, tiled=True)


def local(tokens, norm_gain, gate_weight, up_weight, down_weight):
    f32, bf16 = jnp.float32, jnp.bfloat16
    values = tokens.astype(f32)
    factor = lax.rsqrt(jnp.mean(values * values, axis=-1, keepdims=True) + eps_floor)
    normed = (values * factor * norm_gain).astype(bf16)
    half = normed.shape[0] // 2
    halves = [normed[:half], normed[half:]]

    ahead, behind = {0: halves}, {0: halves}
    for d in (1, 2, 3):
        ahead[d] = [shift(h, 1) for h in ahead[d - 1]]
        behind[d] = [shift(h, -1) for h in behind[d - 1]]
    far = [shift(ahead[3][0], 1), shift(behind[3][1], -1)]

    def whole(w, dim):
        blocks = from_everyone(w, ("y", "x"))
        mine = jnp.moveaxis(blocks, 0, dim)
        mine = mine.reshape(*mine.shape[:dim], -1, *mine.shape[dim + 2 :])
        return mine, swap(mine)

    gates = whole(gate_weight, 0)
    ups = whole(up_weight, 0)
    downs = whole(down_weight, 1)
    gate_up = jnp.concatenate([gates[0], gates[1], ups[0], ups[1]], axis=1)
    down = jnp.concatenate(downs, axis=0)
    units = down.shape[0]

    def share(pieces):
        rows = jnp.concatenate(pieces, axis=0)
        both = jnp.dot(rows, gate_up, preferred_element_type=f32)
        hidden = (jax.nn.silu(both[:, :units]) * both[:, units:]).astype(bf16)
        return jnp.dot(hidden, down, preferred_element_type=f32)

    def cut(part):
        return [part[i : i + half] for i in range(0, part.shape[0], half)]

    part = cut(share(far))
    going_up = [shift(part[0].astype(bf16), 1), None]
    going_down = [None, shift(part[1].astype(bf16), -1)]

    def joined(arrived, own):
        return own if arrived is None else arrived.astype(f32) + own

    for d in (3, 2, 1):
        part = cut(share(behind[d] + ahead[d]))
        going_up = [shift(joined(a, p).astype(bf16), 1) for a, p in zip(going_up, part[:2])]
        going_down = [shift(joined(a, p).astype(bf16), -1) for a, p in zip(going_down, part[2:])]
    part = cut(share(halves))
    out = [p + a.astype(f32) + b.astype(f32) for p, a, b in zip(part, going_up, going_down)]
    return jnp.concatenate(out, axis=0).astype(bf16)


def solution(mesh):
    fine = Mesh(mesh.devices.reshape(4, 4, 8, 2), ("y", "x", "z", "c"))
    fs, tp = ("y", "x"), ("z", "c")
    return jax.shard_map(
        local,
        mesh=fine,
        in_specs=(P(fs + tp, None), P(), P(fs, tp), P(fs, tp), P(tp, fs)),
        out_specs=P(fs + tp, None),
        check_vma=False,
    )
```

```python
import jax
import jax.numpy as jnp
from jax import lax
from jax.sharding import Mesh, PartitionSpec as P

eps_floor = 0.05
X, Y, Z = 4, 4, 8
AXES = ("y", "x", "z", "c")


def place(y, x, z, c):
    return ((y * X + x) * Z + z) * 2 + c


def rows_and_columns():
    along_x = lambda c: [[place(y, x, z, c) for x in range(X)] for y in range(Y) for z in range(Z)]
    along_y = lambda c: [[place(y, x, z, c) for y in range(Y)] for x in range(X) for z in range(Z)]
    return along_x(0) + along_y(1), along_y(0) + along_x(1)


FIRST, SECOND = rows_and_columns()


def onward(x, by):
    pairs = [(2 * z + c, 2 * ((z + (by if c == 0 else -by)) % Z) + c) for z in range(Z) for c in range(2)]
    return lax.ppermute(x, ("z", "c"), pairs)


def swap(x):
    return lax.ppermute(x, "c", [(0, 1), (1, 0)])


def from_four(x, groups):
    return lax.all_to_all(jnp.broadcast_to(x[None], (4, *x.shape)), AXES, 0, 0, axis_index_groups=groups, tiled=True)


def local(tokens, norm_gain, gate_weight, up_weight, down_weight):
    f32, bf16 = jnp.float32, jnp.bfloat16
    units = down_weight.shape[0]
    values = tokens.astype(f32)
    factor = lax.rsqrt(jnp.mean(values * values, axis=-1, keepdims=True) + eps_floor)
    normed = (values * factor * norm_gain).astype(bf16)
    core = lax.axis_index("c")

    own, mate = {0: normed}, {0: swap(normed)}
    for d in (1, 2, 3):
        own[d], mate[d] = onward(own[d - 1], 1), onward(mate[d - 1], 1)
    own[4] = onward(own[3], 1)

    packed = jnp.concatenate([gate_weight.T, up_weight.T, down_weight], axis=0)
    quarter = from_four(packed, FIRST)

    def whole(rows):
        blocks = from_four(quarter[:, rows], SECOND)
        blocks = jnp.where(core == 0, blocks, blocks.swapaxes(0, 1))
        mine = blocks.transpose(2, 0, 1, 3).reshape(blocks.shape[2], -1)
        return mine, swap(mine)

    gate_up = whole(slice(0, 2 * units))
    down = whole(slice(2 * units, 3 * units))

    def share(pieces):
        rows = jnp.concatenate(pieces, axis=0)
        total = 0.0
        for gu, dn in zip(gate_up, down):
            both = lax.dot_general(rows, gu, (((1,), (1,)), ((), ())), preferred_element_type=f32)
            hidden = (jax.nn.silu(both[:, :units]) * both[:, units:]).astype(bf16)
            total = total + jnp.dot(hidden, dn, preferred_element_type=f32)
        n = pieces[0].shape[0]
        return [total[i : i + n] for i in range(0, total.shape[0], n)]

    own4, own3, mate3 = share([own[4], own[3], mate[3]])
    own2, mate2 = share([own[2], mate[2]])
    own1, mate1, own0 = share([own[1], mate[1], own[0]])

    def send(x):
        return onward(x.astype(bf16), -1)

    got_own = send(own4)
    got_mate = send(mate3)
    got_own = send(got_own.astype(f32) + own3)
    got_mate = send(got_mate.astype(f32) + mate2)
    got_own = send(got_own.astype(f32) + own2)
    got_mate = send(got_mate.astype(f32) + mate1)
    got_own = send(got_own.astype(f32) + own1)
    got_mate = swap(got_mate)
    return (own0 + got_own.astype(f32) + got_mate.astype(f32)).astype(bf16)


def solution(mesh):
    fine = Mesh(mesh.devices.reshape(Y, X, Z, 2), AXES)
    fs, tp = ("y", "x"), ("z", "c")
    return jax.shard_map(
        local,
        mesh=fine,
        in_specs=(P(fs + tp, None), P(), P(fs, tp), P(fs, tp), P(tp, fs)),
        out_specs=P(fs + tp, None),
        check_vma=False,
    )
```

```python
import functools

import jax
import jax.numpy as jnp
from jax import lax
from jax.experimental import pallas as pl
from jax.experimental.pallas import tpu as pltpu
from jax.sharding import Mesh, PartitionSpec as P


eps_floor = 0.05
X, Y, Z = 4, 4, 8
AXES = ("y", "x", "z", "c")
LANES = 128
f32, bf16 = jnp.float32, jnp.bfloat16


def place(y, x, z, c):
    return ((y * X + x) * Z + z) * 2 + c


def rows_and_columns():
    along_x = lambda c: [[place(y, x, z, c) for x in range(X)] for y in range(Y) for z in range(Z)]
    along_y = lambda c: [[place(y, x, z, c) for y in range(Y)] for x in range(X) for z in range(Z)]
    return along_x(0) + along_y(1), along_y(0) + along_x(1)


FIRST, SECOND = rows_and_columns()
WHOLE = pl.BlockSpec(memory_space=pltpu.VMEM)
SMALL = pltpu.CompilerParams(vmem_limit_bytes=12 << 20)


def onward(x, by):
    pairs = [(2 * z + c, 2 * ((z + (by if c == 0 else -by)) % Z) + c) for z in range(Z) for c in range(2)]
    return lax.ppermute(x, ("z", "c"), pairs)


def swap(x):
    return lax.ppermute(x, "c", [(0, 1), (1, 0)])


def from_four(copies, groups):
    return lax.all_to_all(copies, AXES, 0, 0, axis_index_groups=groups, tiled=True)


def norm_body(tokens, gain, out):
    values = tokens[...].astype(f32)
    factor = lax.rsqrt(jnp.mean(values * values, axis=-1, keepdims=True) + eps_floor)
    out[...] = (values * factor * gain[...]).T.astype(bf16)


def norm(tokens, gain):
    return pl.pallas_call(
        norm_body,
        out_shape=jax.ShapeDtypeStruct(tokens.shape[::-1], bf16),
        in_specs=[WHOLE, WHOLE],
        out_specs=WHOLE,
        compiler_params=SMALL,
        name="norm",
    )(tokens, gain[None])


def spread_body(units, packed, gate_up, down):
    for k in range(packed.shape[0]):
        gate_up[0, :, LANES * k : LANES * (k + 1)] = packed[k, : 2 * units]
        down[0, LANES * k : LANES * (k + 1), :units] = packed[k, 2 * units :].T
        down[0, LANES * k : LANES * (k + 1), units:] = jnp.zeros((LANES, down.shape[2] - units), bf16)


def spread(packed):
    n, units = packed.shape[0], packed.shape[1] // 3
    shapes = [(n, 2 * units, n * LANES), (n, n * LANES, pl.cdiv(units, LANES) * LANES)]
    return pl.pallas_call(
        functools.partial(spread_body, units),
        grid=(n,),
        out_shape=[jax.ShapeDtypeStruct(s, bf16) for s in shapes],
        in_specs=[pl.BlockSpec(packed.shape, lambda i: (0, 0, 0))],
        out_specs=[pl.BlockSpec((1, *s[1:]), lambda i: (i, 0, 0)) for s in shapes],
        compiler_params=SMALL,
        name="spread",
    )(packed)


def share_body(n, units, core_ref, *refs):
    pieces, weights, outs, turned = refs[:n], refs[n : n + 4], refs[n + 4 : 2 * n + 4], refs[2 * n + 4]
    depth, m = weights[0].shape[2], pieces[0].shape[1]
    blocks = turned.shape[0] // LANES
    core = core_ref[0]

    def order(b, w):
        return jnp.where(core == w, b, (b % 4) * 4 + b // 4)

    hidden = []
    for w in (0, 1):
        for b in range(blocks):
            at = pl.ds(pl.multiple_of(order(b, w) * LANES, LANES), LANES)
            for i in range(n):
                turned[LANES * b : LANES * (b + 1), m * i : m * (i + 1)] = pieces[i][at, :]
        both = jnp.dot(weights[2 * w][0], turned[:depth], preferred_element_type=f32)
        for k in range(1, 4):
            both += jnp.dot(weights[2 * w][k], turned[depth * k : depth * (k + 1)], preferred_element_type=f32)
        gate, upper = both[:units], both[units:]
        hidden.append((gate / (1.0 + jnp.exp(-gate)) * upper).astype(bf16))
    for b in range(blocks):
        part = 0.0
        for w in (0, 1):
            at = order(b, w)
            rows = weights[2 * w + 1][at // 4, pl.ds(pl.multiple_of(at % 4 * LANES, LANES), LANES), :units]
            part += jnp.dot(rows, hidden[w], preferred_element_type=f32)
        for i in range(n):
            outs[i][LANES * b : LANES * (b + 1), :] = part[:, m * i : m * (i + 1)].astype(outs[i].dtype)


def share(core, pieces, weights, dtype):
    n, units = len(pieces), weights[0].shape[1] // 2
    shape = pieces[0].shape
    return pl.pallas_call(
        functools.partial(share_body, n, units),
        out_shape=[jax.ShapeDtypeStruct(shape, dtype)] * n,
        in_specs=[pl.BlockSpec(memory_space=pltpu.SMEM)] + [WHOLE] * (n + 4),
        out_specs=[WHOLE] * n,
        scratch_shapes=[pltpu.VMEM((shape[0], n * shape[1]), bf16)],
        compiler_params=pltpu.CompilerParams(vmem_limit_bytes=24 << 20),
        name="share",
    )(core, *pieces, *weights)


def close_body(own, first, second, out):
    out[...] = (own[...] + first[...].astype(f32) + second[...].astype(f32)).T.astype(bf16)


def close(own, first, second):
    return pl.pallas_call(
        close_body,
        out_shape=jax.ShapeDtypeStruct(own.shape[::-1], bf16),
        in_specs=[WHOLE] * 3,
        out_specs=WHOLE,
        compiler_params=SMALL,
        name="close",
    )(own, first, second)


def local(tokens, norm_gain, gate_weight, up_weight, down_weight):
    core = lax.axis_index("c").astype(jnp.int32)[None]
    normed = norm(tokens, norm_gain)

    own, mate = {0: normed}, {0: swap(normed)}
    for d in (1, 2, 3, 4):
        own[d] = onward(own[d - 1], 1)
        if d < 4:
            mate[d] = onward(mate[d - 1], 1)

    packed = jnp.concatenate([gate_weight.T, up_weight.T, down_weight], axis=0)
    copies = jnp.broadcast_to(packed[None], (4, *packed.shape))
    rows = from_four(copies, FIRST)
    gate_up, down = spread(rows)
    gate_up = from_four(gate_up, SECOND)
    down = from_four(down, SECOND)
    gate_up_mate = swap(gate_up)
    down_mate = swap(down)
    weights = (gate_up, down, gate_up_mate, down_mate)

    own4, mate3 = share(core, [own[4], mate[3]], weights, bf16)
    own3, mate2 = share(core, [own[3], mate[2]], weights, f32)
    own2, mate1 = share(core, [own[2], mate[1]], weights, f32)
    own1, own0 = share(core, [own[1], own[0]], weights, f32)

    def send(x):
        return onward(x.astype(bf16), -1)

    got_own = send(own4)
    got_mate = send(mate3)
    got_own = send(got_own.astype(f32) + own3)
    got_mate = send(got_mate.astype(f32) + mate2)
    got_own = send(got_own.astype(f32) + own2)
    got_mate = send(got_mate.astype(f32) + mate1)
    got_own = send(got_own.astype(f32) + own1)
    return close(own0, got_own, swap(got_mate))


def solution(mesh):
    fine = Mesh(mesh.devices.reshape(Y, X, Z, 2), AXES)
    fs, tp = ("y", "x"), ("z", "c")

    return jax.shard_map(
        local,
        mesh=fine,
        in_specs=(P(fs + tp, None), P(), P(fs, tp), P(fs, tp), P(tp, fs)),
        out_specs=P(fs + tp, None),
        check_vma=False,
    )
```

```python
import functools

import jax
import jax.numpy as jnp
from jax import lax
from jax.experimental import pallas as pl
from jax.experimental.pallas import tpu as pltpu
from jax.sharding import Mesh, PartitionSpec as P


eps_floor = 0.05
X, Y, Z = 4, 4, 8
AXES = ("y", "x", "z", "c")
LANES = 128
f32, bf16 = jnp.float32, jnp.bfloat16


def place(y, x, z, c):
    return ((y * X + x) * Z + z) * 2 + c


def rows_and_columns():
    along_x = lambda c: [[place(y, x, z, c) for x in range(X)] for y in range(Y) for z in range(Z)]
    along_y = lambda c: [[place(y, x, z, c) for y in range(Y)] for x in range(X) for z in range(Z)]
    return along_x(0) + along_y(1), along_y(0) + along_x(1)


FIRST, SECOND = rows_and_columns()
WHOLE = pl.BlockSpec(memory_space=pltpu.VMEM)
LARGE = pltpu.CompilerParams(vmem_limit_bytes=60 << 20)
SMALL = pltpu.CompilerParams(vmem_limit_bytes=12 << 20)


def onward(x, by):
    pairs = [(2 * z + c, 2 * ((z + (by if c == 0 else -by)) % Z) + c) for z in range(Z) for c in range(2)]
    return lax.ppermute(x, ("z", "c"), pairs)


def swap(x):
    return lax.ppermute(x, "c", [(0, 1), (1, 0)])


def from_four(copies, groups):
    return lax.all_to_all(copies, AXES, 0, 0, axis_index_groups=groups, tiled=True)


def norm_body(tokens, gain, out):
    values = tokens[...].astype(f32)
    factor = lax.rsqrt(jnp.mean(values * values, axis=-1, keepdims=True) + eps_floor)
    out[...] = (values * factor * gain[...]).T.astype(bf16)


def norm(tokens, gain):
    return pl.pallas_call(
        norm_body,
        out_shape=jax.ShapeDtypeStruct(tokens.shape[::-1], bf16),
        in_specs=[WHOLE, WHOLE],
        out_specs=WHOLE,
        compiler_params=SMALL,
        name="norm",
    )(tokens, gain[None])


def repeat(packed, out, sems):
    copies = [pltpu.make_async_copy(packed, out.at[k], sems.at[k]) for k in range(4)]
    for c in copies:
        c.start()
    for c in copies:
        c.wait()


def repeated(body, shape, *operands, room=SMALL):
    return pl.pallas_call(
        body,
        out_shape=jax.ShapeDtypeStruct((4, *shape), bf16),
        in_specs=[WHOLE] * len(operands),
        out_specs=pl.BlockSpec(memory_space=pltpu.HBM),
        scratch_shapes=[pltpu.VMEM(shape, bf16), pltpu.SemaphoreType.DMA((4,))],
        compiler_params=room,
    )(*operands)


def pack_body(gate, upper, down, out, packed, sems):
    units = gate.shape[0]
    packed[:units] = gate[...]
    packed[units : 2 * units] = upper[...]
    for at in range(0, units, LANES):
        n = min(LANES, units - at)
        rows = slice(2 * units + at, 2 * units + at + LANES)
        packed[rows, :n] = down[at : at + n].T
        if n < LANES:
            packed[rows, n:] = jnp.zeros((LANES, LANES - n), bf16)
    repeat(packed, out, sems)


def pack(gate, upper, down):
    rows = 2 * gate.shape[0] + pl.cdiv(gate.shape[0], LANES) * LANES
    return repeated(pack_body, (rows, LANES), gate, upper, down)


def spread_body(blocks, out, packed, sems):
    for k in range(4):
        packed[:, LANES * k : LANES * (k + 1)] = blocks[k]
    repeat(packed, out, sems)


def spread(blocks):
    return repeated(spread_body, (blocks.shape[1], 4 * LANES), blocks, room=LARGE)


def hold_body(source, out, sem):
    copy = pltpu.make_async_copy(source, out, sem)
    copy.start()
    copy.wait()


def hold(x):
    return pl.pallas_call(
        hold_body,
        out_shape=jax.ShapeDtypeStruct(x.shape, x.dtype),
        in_specs=[pl.BlockSpec(memory_space=pltpu.HBM)],
        out_specs=WHOLE,
        scratch_shapes=[pltpu.SemaphoreType.DMA],
        compiler_params=SMALL,
        name="hold",
    )(x)


def order(core, b, w):
    return jnp.where(core == w, b, (b % 4) * 4 + b // 4)


def half_hidden(core, w, units, pieces, weights, turned):
    m, depth = pieces[0].shape[1], weights.shape[2]
    for b in range(turned.shape[0] // LANES):
        at = pl.ds(pl.multiple_of(order(core, b, w) * LANES, LANES), LANES)
        for i, piece in enumerate(pieces):
            turned[LANES * b : LANES * (b + 1), m * i : m * (i + 1)] = piece[at, :]
    both = jnp.dot(weights[0, : 2 * units], turned[:depth], preferred_element_type=f32)
    for k in range(1, 4):
        both += jnp.dot(weights[k, : 2 * units], turned[depth * k : depth * (k + 1)], preferred_element_type=f32)
    gate, upper = both[:units], both[units:]
    return (gate / (1.0 + jnp.exp(-gate)) * upper).astype(bf16)


def begin_body(n, units, core_ref, *refs):
    pieces, weights, out, turned = refs[:n], refs[n], refs[n + 1], refs[n + 2]
    out[...] = half_hidden(core_ref[0], 0, units, pieces, weights, turned)


def finish_body(n, units, core_ref, *refs):
    pieces, weights, first, outs, turned = refs[:n], refs[n : n + 2], refs[n + 2], refs[n + 3 : 2 * n + 3], refs[2 * n + 3]
    core, m = core_ref[0], pieces[0].shape[1]
    hidden = first[...], half_hidden(core, 1, units, pieces, weights[1], turned)
    for b in range(turned.shape[0] // LANES):
        part = 0.0
        for w in (0, 1):
            at = order(core, b, w)
            lanes = pl.ds(pl.multiple_of(at % 4 * LANES, LANES), LANES)
            tiles = [weights[w][at // 4, r : r + LANES, lanes] for r in range(2 * units, weights[w].shape[1], LANES)]
            part += jnp.dot(jnp.concatenate(tiles, axis=1)[:, :units], hidden[w], preferred_element_type=f32)
        for i in range(n):
            outs[i][LANES * b : LANES * (b + 1), :] = part[:, m * i : m * (i + 1)].astype(outs[i].dtype)


def call(body, units, core, pieces, rest, out_shape):
    n, (features, m) = len(pieces), pieces[0].shape
    return pl.pallas_call(
        functools.partial(body, n, units),
        out_shape=out_shape,
        in_specs=[pl.BlockSpec(memory_space=pltpu.SMEM)] + [WHOLE] * (n + len(rest)),
        out_specs=jax.tree.map(lambda _: WHOLE, out_shape),
        scratch_shapes=[pltpu.VMEM((features, n * m), bf16)],
        compiler_params=pltpu.CompilerParams(vmem_limit_bytes=18 << 20),
    )(core, *pieces, *rest)


def begin(units, core, pieces, weights):
    n, m = len(pieces), pieces[0].shape[1]
    return call(begin_body, units, core, pieces, [weights], jax.ShapeDtypeStruct((units, n * m), bf16))


def finish(units, core, pieces, weights, first, dtype):
    out_shape = [jax.ShapeDtypeStruct(p.shape, dtype) for p in pieces]
    return call(finish_body, units, core, pieces, [*weights, first], out_shape)


def close_body(own, first, second, out):
    out[...] = (own[...] + first[...].astype(f32) + second[...].astype(f32)).T.astype(bf16)


def close(own, first, second):
    return pl.pallas_call(
        close_body,
        out_shape=jax.ShapeDtypeStruct(own.shape[::-1], bf16),
        in_specs=[WHOLE] * 3,
        out_specs=WHOLE,
        compiler_params=SMALL,
        name="close",
    )(own, first, second)


def local(tokens, norm_gain, gate_weight, up_weight, down_weight):
    core = lax.axis_index("c").astype(jnp.int32)[None]
    normed = norm(tokens, norm_gain)

    own, mate = {0: normed}, {0: swap(normed)}
    for d in (1, 2, 3, 4):
        own[d] = onward(own[d - 1], 1)
        if d < 4:
            mate[d] = onward(mate[d - 1], 1)

    rows = from_four(pack(gate_weight.T, up_weight.T, down_weight), FIRST)
    columns = from_four(spread(rows), SECOND)
    other = swap(columns)
    columns = hold(columns)
    weights = columns, hold(other)

    units = down_weight.shape[0]
    groups = [(own[4], mate[3]), (own[3], mate[2]), (own[2], mate[1]), (own[1], own[0])]
    firsts = []
    for g in groups:
        firsts.append(begin(units, core, g, columns))
    dtypes = [bf16, f32, f32, f32]
    shares = [finish(units, core, g, weights, f, t) for g, f, t in zip(groups, firsts, dtypes)]
    (own4, mate3), (own3, mate2), (own2, mate1), (own1, own0) = shares

    def send(x):
        return onward(x.astype(bf16), -1)

    got_own = send(own4)
    got_mate = send(mate3)
    got_own = send(got_own.astype(f32) + own3)
    got_mate = send(got_mate.astype(f32) + mate2)
    got_own = send(got_own.astype(f32) + own2)
    got_mate = send(got_mate.astype(f32) + mate1)
    got_own = send(got_own.astype(f32) + own1)
    return close(own0, got_own, swap(got_mate))


def solution(mesh):
    fine = Mesh(mesh.devices.reshape(Y, X, Z, 2), AXES)
    fs, tp = ("y", "x"), ("z", "c")

    return jax.shard_map(
        local,
        mesh=fine,
        in_specs=(P(fs + tp, None), P(), P(fs, tp), P(fs, tp), P(tp, fs)),
        out_specs=P(fs + tp, None),
        check_vma=False,
    )
```

```python
import functools

import jax
import jax.numpy as jnp
from jax import lax
from jax.experimental import pallas as pl
from jax.experimental.pallas import tpu as pltpu
from jax.sharding import Mesh, PartitionSpec as P


eps_floor = 0.05
X, Y, Z = 4, 4, 8
AXES = ("y", "x", "z", "c")
LANES = 128
f32, bf16 = jnp.float32, jnp.bfloat16


def place(y, x, z, c):
    return ((y * X + x) * Z + z) * 2 + c


ROWS = [[place(y, x, z, 0) for x in range(X)] for y in range(Y) for z in range(Z)]
ROWS += [[place(y, x, z, 1) for y in range(Y)] for x in range(X) for z in range(Z)]
WHOLE = pl.BlockSpec(memory_space=pltpu.VMEM)
SMALL = pltpu.CompilerParams(vmem_limit_bytes=12 << 20)


def onward(x, by):
    pairs = [(2 * z + c, 2 * ((z + (by if c == 0 else -by)) % Z) + c) for z in range(Z) for c in range(2)]
    return lax.ppermute(x, ("z", "c"), pairs)


def along_column(x, by):
    flat = lambda y, x, c: (y % Y * X + x % X) * 2 + c
    pairs = [(flat(j, i, 0), flat(j + by, i, 0)) for j in range(Y) for i in range(X)]
    pairs += [(flat(j, i, 1), flat(j, i + by, 1)) for j in range(Y) for i in range(X)]
    return lax.ppermute(x, ("y", "x", "c"), pairs)


def swap(x):
    return lax.ppermute(x, "c", [(0, 1), (1, 0)])


def from_four(copies, groups):
    return lax.all_to_all(copies, AXES, 0, 0, axis_index_groups=groups, tiled=True)


def norm_body(tokens, gain, out):
    values = tokens[...].astype(f32)
    factor = lax.rsqrt(jnp.mean(values * values, axis=-1, keepdims=True) + eps_floor)
    out[...] = (values * factor * gain[...]).T.astype(bf16)


def norm(tokens, gain):
    return pl.pallas_call(
        norm_body,
        out_shape=jax.ShapeDtypeStruct(tokens.shape[::-1], bf16),
        in_specs=[WHOLE, WHOLE],
        out_specs=WHOLE,
        compiler_params=SMALL,
        name="norm",
    )(tokens, gain[None])


def repeat(packed, out, sems):
    copies = [pltpu.make_async_copy(packed, out.at[k], sems.at[k]) for k in range(4)]
    for c in copies:
        c.start()
    for c in copies:
        c.wait()


def repeated(body, shape, *operands):
    return pl.pallas_call(
        body,
        out_shape=jax.ShapeDtypeStruct((4, *shape), bf16),
        in_specs=[WHOLE] * len(operands),
        out_specs=pl.BlockSpec(memory_space=pltpu.HBM),
        scratch_shapes=[pltpu.VMEM(shape, bf16), pltpu.SemaphoreType.DMA((4,))],
        compiler_params=SMALL,
    )(*operands)


def pack_body(gate, upper, down, out, packed, sems):
    units = gate.shape[0]
    packed[:units] = gate[...]
    packed[units : 2 * units] = upper[...]
    for at in range(0, units, LANES):
        n = min(LANES, units - at)
        rows = slice(2 * units + at, 2 * units + at + LANES)
        packed[rows, :n] = down[at : at + n].T
        if n < LANES:
            packed[rows, n:] = jnp.zeros((LANES, LANES - n), bf16)
    repeat(packed, out, sems)


def pack(gate, upper, down):
    rows = 2 * gate.shape[0] + pl.cdiv(gate.shape[0], LANES) * LANES
    return repeated(pack_body, (rows, LANES), gate, upper, down)


def spread_body(blocks, out):
    for k in range(4):
        out[:, LANES * k : LANES * (k + 1)] = blocks[k]


def spread(blocks):
    return pl.pallas_call(
        spread_body,
        out_shape=jax.ShapeDtypeStruct((blocks.shape[1], 4 * LANES), bf16),
        in_specs=[WHOLE],
        out_specs=WHOLE,
        compiler_params=SMALL,
        name="spread",
    )(blocks)


def hold_body(place_ref, here, before, after, top, bottom, out, sems):
    at, half = place_ref[0], top.shape[0]
    ends = [
        (here, out.at[at]),
        (before, out.at[(at + 3) % 4]),
        (after, out.at[(at + 1) % 4]),
        (top, out.at[(at + 2) % 4, :half]),
        (bottom, out.at[(at + 2) % 4, half:]),
    ]
    copies = [pltpu.make_async_copy(*e, sems.at[i]) for i, e in enumerate(ends)]
    for c in copies:
        c.start()
    for c in copies:
        c.wait()


def hold(place, blocks):
    return pl.pallas_call(
        hold_body,
        out_shape=jax.ShapeDtypeStruct((4, *blocks[0].shape), bf16),
        in_specs=[pl.BlockSpec(memory_space=pltpu.SMEM)] + [pl.BlockSpec(memory_space=pltpu.HBM)] * 5,
        out_specs=WHOLE,
        scratch_shapes=[pltpu.SemaphoreType.DMA((5,))],
        compiler_params=SMALL,
        name="hold",
    )(place, *blocks)


def order(core, b, w):
    return jnp.where(core == w, b, (b % 4) * 4 + b // 4)


def half_hidden(core, w, units, pieces, weights, turned):
    m, depth = pieces[0].shape[1], weights.shape[2]
    for b in range(turned.shape[0] // LANES):
        at = pl.ds(pl.multiple_of(order(core, b, w) * LANES, LANES), LANES)
        for i, piece in enumerate(pieces):
            turned[LANES * b : LANES * (b + 1), m * i : m * (i + 1)] = piece[at, :]
    both = jnp.dot(weights[0, : 2 * units], turned[:depth], preferred_element_type=f32)
    for k in range(1, 4):
        both += jnp.dot(weights[k, : 2 * units], turned[depth * k : depth * (k + 1)], preferred_element_type=f32)
    gate, upper = both[:units], both[units:]
    return (gate / (1.0 + jnp.exp(-gate)) * upper).astype(bf16)


def begin_body(n, units, core_ref, *refs):
    pieces, weights, out, turned = refs[:n], refs[n], refs[n + 1], refs[n + 2]
    out[...] = half_hidden(core_ref[0], 0, units, pieces, weights, turned)


def finish_body(n, units, core_ref, *refs):
    pieces, weights, first, outs, turned = refs[:n], refs[n : n + 2], refs[n + 2], refs[n + 3 : 2 * n + 3], refs[2 * n + 3]
    core, m = core_ref[0], pieces[0].shape[1]
    hidden = first[...], half_hidden(core, 1, units, pieces, weights[1], turned)
    for b in range(turned.shape[0] // LANES):
        part = 0.0
        for w in (0, 1):
            at = order(core, b, w)
            lanes = pl.ds(pl.multiple_of(at % 4 * LANES, LANES), LANES)
            tiles = [weights[w][at // 4, r : r + LANES, lanes] for r in range(2 * units, weights[w].shape[1], LANES)]
            part += jnp.dot(jnp.concatenate(tiles, axis=1)[:, :units], hidden[w], preferred_element_type=f32)
        for i in range(n):
            outs[i][LANES * b : LANES * (b + 1), :] = part[:, m * i : m * (i + 1)].astype(outs[i].dtype)


def call(body, units, core, pieces, rest, out_shape):
    n, (features, m) = len(pieces), pieces[0].shape
    return pl.pallas_call(
        functools.partial(body, n, units),
        out_shape=out_shape,
        in_specs=[pl.BlockSpec(memory_space=pltpu.SMEM)] + [WHOLE] * (n + len(rest)),
        out_specs=jax.tree.map(lambda _: WHOLE, out_shape),
        scratch_shapes=[pltpu.VMEM((features, n * m), bf16)],
        compiler_params=pltpu.CompilerParams(vmem_limit_bytes=18 << 20),
    )(core, *pieces, *rest)


def begin(units, core, pieces, weights):
    n, m = len(pieces), pieces[0].shape[1]
    return call(begin_body, units, core, pieces, [weights], jax.ShapeDtypeStruct((units, n * m), bf16))


def finish(units, core, pieces, weights, first, dtype):
    out_shape = [jax.ShapeDtypeStruct(p.shape, dtype) for p in pieces]
    return call(finish_body, units, core, pieces, [*weights, first], out_shape)


def close_body(own, first, second, out):
    out[...] = (own[...] + first[...].astype(f32) + second[...].astype(f32)).T.astype(bf16)


def close(own, first, second):
    return pl.pallas_call(
        close_body,
        out_shape=jax.ShapeDtypeStruct(own.shape[::-1], bf16),
        in_specs=[WHOLE] * 3,
        out_specs=WHOLE,
        compiler_params=SMALL,
        name="close",
    )(own, first, second)


def local(tokens, norm_gain, gate_weight, up_weight, down_weight):
    core = lax.axis_index("c").astype(jnp.int32)[None]
    normed = norm(tokens, norm_gain)

    own, mate = {0: normed}, {0: swap(normed)}
    for d in (1, 2, 3, 4):
        own[d] = onward(own[d - 1], 1)
        if d < 4:
            mate[d] = onward(mate[d - 1], 1)

    rows = from_four(pack(gate_weight.T, up_weight.T, down_weight), ROWS)
    here = spread(rows)
    half = here.shape[0] // 2
    before = along_column(here, 1)
    after = along_column(here, -1)
    top = along_column(before[:half], 1)
    bottom = along_column(after[half:], -1)
    blocks = here, before, after, top, bottom
    others = []
    for b in blocks:
        others.append(swap(b))
    row, column = lax.axis_index("y").astype(jnp.int32)[None], lax.axis_index("x").astype(jnp.int32)[None]
    first = core == 0
    columns = hold(jnp.where(first, row, column), blocks)
    weights = columns, hold(jnp.where(first, column, row), others)

    units = down_weight.shape[0]
    groups = [(own[4], mate[3]), (own[3], mate[2]), (own[2], mate[1]), (own[1], own[0])]
    firsts = []
    for g in groups:
        firsts.append(begin(units, core, g, columns))
    dtypes = [bf16, f32, f32, f32]
    shares = [finish(units, core, g, weights, f, t) for g, f, t in zip(groups, firsts, dtypes)]
    (own4, mate3), (own3, mate2), (own2, mate1), (own1, own0) = shares

    def send(x):
        return onward(x.astype(bf16), -1)

    got_own = send(own4)
    got_mate = send(mate3)
    got_own = send(got_own.astype(f32) + own3)
    got_mate = send(got_mate.astype(f32) + mate2)
    got_own = send(got_own.astype(f32) + own2)
    got_mate = send(got_mate.astype(f32) + mate1)
    got_own = send(got_own.astype(f32) + own1)
    return close(own0, got_own, swap(got_mate))


def solution(mesh):
    fine = Mesh(mesh.devices.reshape(Y, X, Z, 2), AXES)
    fs, tp = ("y", "x"), ("z", "c")

    return jax.shard_map(
        local,
        mesh=fine,
        in_specs=(P(fs + tp, None), P(), P(fs, tp), P(fs, tp), P(tp, fs)),
        out_specs=P(fs + tp, None),
        check_vma=False,
    )
```

```python
import functools

import jax
import jax.numpy as jnp
from jax import lax
from jax.experimental import pallas as pl
from jax.experimental.pallas import tpu as pltpu
from jax.sharding import Mesh, PartitionSpec as P


eps_floor = 0.05
X, Y, Z = 4, 4, 8
AXES = ("y", "x", "z", "c")
LANES = 128
f32, bf16 = jnp.float32, jnp.bfloat16


def place(y, x, z, c):
    return ((y * X + x) * Z + z) * 2 + c


ROWS = [[place(y, x, z, 0) for x in range(X)] for y in range(Y) for z in range(Z)]
ROWS += [[place(y, x, z, 1) for y in range(Y)] for x in range(X) for z in range(Z)]
WHOLE = pl.BlockSpec(memory_space=pltpu.VMEM)
FULL = pltpu.CompilerParams(vmem_limit_bytes=67_000_000)
SMALL = pltpu.CompilerParams(vmem_limit_bytes=12 << 20)


def onward(x, by):
    pairs = [(2 * z + c, 2 * ((z + (by if c == 0 else -by)) % Z) + c) for z in range(Z) for c in range(2)]
    return lax.ppermute(x, ("z", "c"), pairs)


def along_column(x, by):
    flat = lambda y, x, c: (y % Y * X + x % X) * 2 + c
    pairs = [(flat(j, i, 0), flat(j + by, i, 0)) for j in range(Y) for i in range(X)]
    pairs += [(flat(j, i, 1), flat(j, i + by, 1)) for j in range(Y) for i in range(X)]
    return lax.ppermute(x, ("y", "x", "c"), pairs)


def swap(x):
    return lax.ppermute(x, "c", [(0, 1), (1, 0)])


def from_four(copies, groups):
    return lax.all_to_all(copies, AXES, 0, 0, axis_index_groups=groups, tiled=True)


def norm_body(tokens_in, gain_in, out, tokens, gain, sems):
    copies = [pltpu.make_async_copy(tokens_in, tokens, sems.at[0]), pltpu.make_async_copy(gain_in, gain, sems.at[1])]
    for c in copies:
        c.start()
    for c in copies:
        c.wait()
    values = tokens[...].astype(f32)
    factor = lax.rsqrt(jnp.mean(values * values, axis=-1, keepdims=True) + eps_floor)
    out[...] = (values * factor * gain[...]).T.astype(bf16)


def norm(tokens, gain):
    return pl.pallas_call(
        norm_body,
        out_shape=jax.ShapeDtypeStruct(tokens.shape[::-1], bf16),
        in_specs=[pl.BlockSpec(memory_space=pltpu.HBM)] * 2,
        out_specs=WHOLE,
        scratch_shapes=[
            pltpu.VMEM(tokens.shape, bf16),
            pltpu.VMEM((1, tokens.shape[1]), f32),
            pltpu.SemaphoreType.DMA((2,)),
        ],
        compiler_params=FULL,
        name="norm",
    )(tokens, gain[None])


def pack_body(gate_in, upper_in, down_in, out, packed, down, sems):
    units = gate_in.shape[0]
    into = [
        pltpu.make_async_copy(gate_in, packed.at[:units], sems.at[0]),
        pltpu.make_async_copy(upper_in, packed.at[units : 2 * units], sems.at[1]),
        pltpu.make_async_copy(down_in, down, sems.at[2]),
    ]
    for c in into:
        c.start()
    for c in into:
        c.wait()
    for at in range(0, units, LANES):
        n = min(LANES, units - at)
        rows = slice(2 * units + at, 2 * units + at + LANES)
        packed[rows, :n] = down[at : at + n].T
        if n < LANES:
            packed[rows, n:] = jnp.zeros((LANES, LANES - n), bf16)
    copies = [pltpu.make_async_copy(packed, out.at[k], sems.at[3 + k]) for k in range(4)]
    for c in copies:
        c.start()
    for c in copies:
        c.wait()


def pack(gate, upper, down):
    units = gate.shape[0]
    shape = (2 * units + pl.cdiv(units, LANES) * LANES, LANES)
    return pl.pallas_call(
        pack_body,
        out_shape=jax.ShapeDtypeStruct((4, *shape), bf16),
        in_specs=[pl.BlockSpec(memory_space=pltpu.HBM)] * 3,
        out_specs=pl.BlockSpec(memory_space=pltpu.HBM),
        scratch_shapes=[pltpu.VMEM(shape, bf16), pltpu.VMEM(down.shape, bf16), pltpu.SemaphoreType.DMA((7,))],
        compiler_params=FULL,
        name="pack",
    )(gate, upper, down)


def spread_body(blocks, *halves):
    n = halves[0].shape[0]
    for i, out in enumerate(halves):
        for k in range(4):
            out[:, LANES * k : LANES * (k + 1)] = blocks[k, n * i : n * (i + 1)]


def spread(blocks):
    return pl.pallas_call(
        spread_body,
        out_shape=[jax.ShapeDtypeStruct((blocks.shape[1] // 2, 4 * LANES), bf16)] * 2,
        in_specs=[WHOLE],
        out_specs=[WHOLE] * 2,
        compiler_params=SMALL,
        name="spread",
    )(blocks)


def hold_body(place_ref, *refs):
    blocks, out, sems = refs[:8], refs[8], refs[9]
    at, half = place_ref[0], blocks[0].shape[0]
    copies = []
    for i, b in enumerate(blocks):
        end = out.at[(at + (0, 3, 1, 2)[i // 2]) % 4, half * (i % 2) : half * (i % 2 + 1)]
        copies.append(pltpu.make_async_copy(b, end, sems.at[i]))
    for c in copies:
        c.start()
    for c in copies:
        c.wait()


def hold(place, blocks):
    half, width = blocks[0].shape
    return pl.pallas_call(
        hold_body,
        out_shape=jax.ShapeDtypeStruct((4, 2 * half, width), bf16),
        in_specs=[pl.BlockSpec(memory_space=pltpu.SMEM)] + [pl.BlockSpec(memory_space=pltpu.HBM)] * 8,
        out_specs=WHOLE,
        scratch_shapes=[pltpu.SemaphoreType.DMA((8,))],
        compiler_params=SMALL,
        name="hold",
    )(place, *blocks)


def order(core, b, w):
    return jnp.where(core == w, b, (b % 4) * 4 + b // 4)


def half_hidden(core, w, units, pieces, weights, turned):
    m, depth = pieces[0].shape[1], weights.shape[2]
    for b in range(turned.shape[0] // LANES):
        at = pl.ds(pl.multiple_of(order(core, b, w) * LANES, LANES), LANES)
        for i, piece in enumerate(pieces):
            turned[LANES * b : LANES * (b + 1), m * i : m * (i + 1)] = piece[at, :]
    both = jnp.dot(weights[0, : 2 * units], turned[:depth], preferred_element_type=f32)
    for k in range(1, 4):
        both += jnp.dot(weights[k, : 2 * units], turned[depth * k : depth * (k + 1)], preferred_element_type=f32)
    gate, upper = both[:units], both[units:]
    return (gate / (1.0 + jnp.exp(-gate)) * upper).astype(bf16)


def begin_body(n, units, core_ref, *refs):
    pieces, weights, out, turned = refs[:n], refs[n], refs[n + 1], refs[n + 2]
    out[...] = half_hidden(core_ref[0], 0, units, pieces, weights, turned)


def finish_body(n, units, core_ref, *refs):
    pieces, weights, first, outs, turned = refs[:n], refs[n : n + 2], refs[n + 2], refs[n + 3 : 2 * n + 3], refs[2 * n + 3]
    core, m = core_ref[0], pieces[0].shape[1]
    hidden = first[...], half_hidden(core, 1, units, pieces, weights[1], turned)
    for b in range(turned.shape[0] // LANES):
        part = 0.0
        for w in (0, 1):
            at = order(core, b, w)
            lanes = pl.ds(pl.multiple_of(at % 4 * LANES, LANES), LANES)
            tiles = [weights[w][at // 4, r : r + LANES, lanes] for r in range(2 * units, weights[w].shape[1], LANES)]
            part += jnp.dot(jnp.concatenate(tiles, axis=1)[:, :units], hidden[w], preferred_element_type=f32)
        for i in range(n):
            outs[i][LANES * b : LANES * (b + 1), :] = part[:, m * i : m * (i + 1)].astype(outs[i].dtype)


def call(body, units, core, pieces, rest, out_shape):
    n, (features, m) = len(pieces), pieces[0].shape
    return pl.pallas_call(
        functools.partial(body, n, units),
        out_shape=out_shape,
        in_specs=[pl.BlockSpec(memory_space=pltpu.SMEM)] + [WHOLE] * (n + len(rest)),
        out_specs=jax.tree.map(lambda _: WHOLE, out_shape),
        scratch_shapes=[pltpu.VMEM((features, n * m), bf16)],
        compiler_params=pltpu.CompilerParams(vmem_limit_bytes=18 << 20),
    )(core, *pieces, *rest)


def begin(units, core, pieces, weights):
    n, m = len(pieces), pieces[0].shape[1]
    return call(begin_body, units, core, pieces, [weights], jax.ShapeDtypeStruct((units, n * m), bf16))


def finish(units, core, pieces, weights, first, dtype):
    out_shape = [jax.ShapeDtypeStruct(p.shape, dtype) for p in pieces]
    return call(finish_body, units, core, pieces, [*weights, first], out_shape)


def close_body(own, first, second, out):
    out[...] = (own[...] + first[...].astype(f32) + second[...].astype(f32)).T.astype(bf16)


def close(own, first, second):
    return pl.pallas_call(
        close_body,
        out_shape=jax.ShapeDtypeStruct(own.shape[::-1], bf16),
        in_specs=[WHOLE] * 3,
        out_specs=WHOLE,
        compiler_params=SMALL,
        name="close",
    )(own, first, second)


def local(tokens, norm_gain, gate_weight, up_weight, down_weight):
    core = lax.axis_index("c").astype(jnp.int32)[None]
    normed = norm(tokens, norm_gain)

    own, mate = {0: normed}, {0: swap(normed)}
    for d in (1, 2, 3, 4):
        own[d] = onward(own[d - 1], 1)
        if d < 4:
            mate[d] = onward(mate[d - 1], 1)

    rows = from_four(pack(gate_weight.T, up_weight.T, down_weight), ROWS)
    top, bottom = spread(rows)
    before_top = along_column(top, 1)
    after_bottom = along_column(bottom, -1)
    before_bottom = along_column(bottom, 1)
    after_top = along_column(top, -1)
    far_top = along_column(before_top, 1)
    far_bottom = along_column(after_bottom, -1)
    blocks = top, bottom, before_top, before_bottom, after_top, after_bottom, far_top, far_bottom
    others = []
    for b in blocks:
        others.append(swap(b))
    row, column = lax.axis_index("y").astype(jnp.int32)[None], lax.axis_index("x").astype(jnp.int32)[None]
    first = core == 0
    columns = hold(jnp.where(first, row, column), blocks)
    weights = columns, hold(jnp.where(first, column, row), others)

    units = down_weight.shape[0]
    groups = [(own[4], mate[3]), (own[3], mate[2]), (own[2], mate[1]), (own[1], own[0])]
    firsts = []
    for g in groups:
        firsts.append(begin(units, core, g, columns))
    dtypes = [bf16, f32, f32, f32]
    shares = [finish(units, core, g, weights, f, t) for g, f, t in zip(groups, firsts, dtypes)]
    (own4, mate3), (own3, mate2), (own2, mate1), (own1, own0) = shares

    def send(x):
        return onward(x.astype(bf16), -1)

    got_own = send(own4)
    got_mate = send(mate3)
    got_own = send(got_own.astype(f32) + own3)
    got_mate = send(got_mate.astype(f32) + mate2)
    got_own = send(got_own.astype(f32) + own2)
    got_mate = send(got_mate.astype(f32) + mate1)
    got_own = send(got_own.astype(f32) + own1)
    return close(own0, got_own, swap(got_mate))


def solution(mesh):
    fine = Mesh(mesh.devices.reshape(Y, X, Z, 2), AXES)
    fs, tp = ("y", "x"), ("z", "c")

    return jax.shard_map(
        local,
        mesh=fine,
        in_specs=(P(fs + tp, None), P(), P(fs, tp), P(fs, tp), P(tp, fs)),
        out_specs=P(fs + tp, None),
        check_vma=False,
    )
```

```python
import functools

import jax
import jax.numpy as jnp
from jax import lax
from jax.experimental import pallas as pl
from jax.experimental.pallas import tpu as pltpu
from jax.sharding import Mesh, PartitionSpec as P


eps_floor = 0.05
X, Y, Z = 4, 4, 8
AXES = ("y", "x", "z", "c")
LANES = 128
f32, bf16 = jnp.float32, jnp.bfloat16


def place(y, x, z, c):
    return ((y * X + x) * Z + z) * 2 + c


ROWS = [[place(y, x, z, 0) for x in range(X)] for y in range(Y) for z in range(Z)]
ROWS += [[place(y, x, z, 1) for y in range(Y)] for x in range(X) for z in range(Z)]
WHOLE = pl.BlockSpec(memory_space=pltpu.VMEM)
FULL = pltpu.CompilerParams(vmem_limit_bytes=67_000_000)
SMALL = pltpu.CompilerParams(vmem_limit_bytes=12 << 20)


def onward(x, by):
    pairs = [(2 * z + c, 2 * ((z + (by if c == 0 else -by)) % Z) + c) for z in range(Z) for c in range(2)]
    return lax.ppermute(x, ("z", "c"), pairs)


def along_column(x, by):
    flat = lambda y, x, c: (y % Y * X + x % X) * 2 + c
    pairs = [(flat(j, i, 0), flat(j + by, i, 0)) for j in range(Y) for i in range(X)]
    pairs += [(flat(j, i, 1), flat(j, i + by, 1)) for j in range(Y) for i in range(X)]
    return lax.ppermute(x, ("y", "x", "c"), pairs)


def swap(x):
    return lax.ppermute(x, "c", [(0, 1), (1, 0)])


def from_four(copies, groups):
    return lax.all_to_all(copies, AXES, 0, 0, axis_index_groups=groups, tiled=True)


def norm_body(tokens_in, gain_in, out, tokens, gain, sems):
    copies = [pltpu.make_async_copy(tokens_in, tokens, sems.at[0]), pltpu.make_async_copy(gain_in, gain, sems.at[1])]
    for c in copies:
        c.start()
    for c in copies:
        c.wait()
    values = tokens[...].astype(f32)
    factor = lax.rsqrt(jnp.mean(values * values, axis=-1, keepdims=True) + eps_floor)
    out[...] = (values * factor * gain[...]).T.astype(bf16)


def norm(tokens, gain):
    return pl.pallas_call(
        norm_body,
        out_shape=jax.ShapeDtypeStruct(tokens.shape[::-1], bf16),
        in_specs=[pl.BlockSpec(memory_space=pltpu.HBM)] * 2,
        out_specs=WHOLE,
        scratch_shapes=[
            pltpu.VMEM(tokens.shape, bf16),
            pltpu.VMEM((1, tokens.shape[1]), f32),
            pltpu.SemaphoreType.DMA((2,)),
        ],
        compiler_params=FULL,
        name="norm",
    )(tokens, gain[None])


def pack_body(gate_in, upper_in, down_in, out, packed, down, sems):
    units = gate_in.shape[0]
    into = [
        pltpu.make_async_copy(gate_in, packed.at[:units], sems.at[0]),
        pltpu.make_async_copy(upper_in, packed.at[units : 2 * units], sems.at[1]),
        pltpu.make_async_copy(down_in, down, sems.at[2]),
    ]
    for c in into:
        c.start()
    for c in into:
        c.wait()
    for at in range(0, units, LANES):
        n = min(LANES, units - at)
        rows = slice(2 * units + at, 2 * units + at + LANES)
        packed[rows, :n] = down[at : at + n].T
        if n < LANES:
            packed[rows, n:] = jnp.zeros((LANES, LANES - n), bf16)
    copies = [pltpu.make_async_copy(packed, out.at[k], sems.at[3 + k]) for k in range(4)]
    for c in copies:
        c.start()
    for c in copies:
        c.wait()


def pack(gate, upper, down):
    units = gate.shape[0]
    shape = (2 * units + pl.cdiv(units, LANES) * LANES, LANES)
    return pl.pallas_call(
        pack_body,
        out_shape=jax.ShapeDtypeStruct((4, *shape), bf16),
        in_specs=[pl.BlockSpec(memory_space=pltpu.HBM)] * 3,
        out_specs=pl.BlockSpec(memory_space=pltpu.HBM),
        scratch_shapes=[pltpu.VMEM(shape, bf16), pltpu.VMEM(down.shape, bf16), pltpu.SemaphoreType.DMA((7,))],
        compiler_params=FULL,
        name="pack",
    )(gate, upper, down)


def spread_body(blocks, whole, *halves):
    n = halves[0].shape[0]
    for i, out in enumerate(halves):
        for k in range(4):
            part = blocks[k, n * i : n * (i + 1)]
            out[:, LANES * k : LANES * (k + 1)] = part
            whole[n * i : n * (i + 1), LANES * k : LANES * (k + 1)] = part


def spread(blocks):
    return pl.pallas_call(
        spread_body,
        out_shape=[jax.ShapeDtypeStruct((blocks.shape[1] // n, 4 * LANES), bf16) for n in (1, 2, 2)],
        in_specs=[WHOLE],
        out_specs=[WHOLE] * 3,
        compiler_params=SMALL,
        name="spread",
    )(blocks)


PARTS = ((0, None), (3, 0), (3, 1), (1, 0), (1, 1), (2, 0), (2, 1))


def hold_body(parts, place_ref, *refs):
    n = len(parts)
    blocks, out, sems = refs[:n], refs[-2], refs[-1]
    half, at = out.shape[1] // 2, place_ref[0]
    copies = []
    for i, (by, h) in enumerate(parts):
        end = out.at[(at + by) % 4] if h is None else out.at[(at + by) % 4, half * h : half * (h + 1)]
        copies.append(pltpu.make_async_copy(blocks[i], end, sems.at[i]))
    for c in copies:
        c.start()
    for c in copies:
        c.wait()


def hold(place, parts, blocks, shape, so_far=None):
    n = len(parts)
    more = [] if so_far is None else [so_far]
    return pl.pallas_call(
        functools.partial(hold_body, parts),
        out_shape=jax.ShapeDtypeStruct(shape, bf16),
        in_specs=[pl.BlockSpec(memory_space=pltpu.SMEM)] + [pl.BlockSpec(memory_space=pltpu.HBM)] * n + [WHOLE] * len(more),
        out_specs=WHOLE,
        input_output_aliases={n + 1: 0} if more else {},
        scratch_shapes=[pltpu.SemaphoreType.DMA((n,))],
        compiler_params=SMALL,
        name="hold",
    )(place, *blocks, *more)


def order(core, b, w):
    return jnp.where(core == w, b, (b % 4) * 4 + b // 4)


def half_hidden(core, w, units, pieces, weights, turned):
    m, depth = pieces[0].shape[1], weights.shape[2]
    for b in range(turned.shape[0] // LANES):
        at = pl.ds(pl.multiple_of(order(core, b, w) * LANES, LANES), LANES)
        for i, piece in enumerate(pieces):
            turned[LANES * b : LANES * (b + 1), m * i : m * (i + 1)] = piece[at, :]
    both = jnp.dot(weights[0, : 2 * units], turned[:depth], preferred_element_type=f32)
    for k in range(1, 4):
        both += jnp.dot(weights[k, : 2 * units], turned[depth * k : depth * (k + 1)], preferred_element_type=f32)
    gate, upper = both[:units], both[units:]
    return (gate / (1.0 + jnp.exp(-gate)) * upper).astype(bf16)


def begin_body(n, units, core_ref, *refs):
    pieces, weights, out, turned = refs[:n], refs[n], refs[n + 1], refs[n + 2]
    out[...] = half_hidden(core_ref[0], 0, units, pieces, weights, turned)


def finish_body(n, units, core_ref, *refs):
    pieces, weights, first = refs[:n], refs[n : n + 2], refs[n + 2]
    outs, turned, held = refs[n + 3 : 2 * n + 3], refs[2 * n + 3], refs[2 * n + 4]
    core, m = core_ref[0], pieces[0].shape[1]
    hidden = first, held
    held[...] = half_hidden(core, 1, units, pieces, weights[1], turned)

    def four(group, carry):
        for j in range(4):
            b = group * 4 + j
            part = 0.0
            for w in (0, 1):
                at = order(core, b, w)
                lanes = pl.ds(pl.multiple_of(at % 4 * LANES, LANES), LANES)
                tiles = [weights[w][at // 4, r : r + LANES, lanes] for r in range(2 * units, weights[w].shape[1], LANES)]
                part += jnp.dot(jnp.concatenate(tiles, axis=1)[:, :units], hidden[w][...], preferred_element_type=f32)
            rows = pl.ds(pl.multiple_of(b * LANES, LANES), LANES)
            for i in range(n):
                outs[i][rows, :] = part[:, m * i : m * (i + 1)].astype(outs[i].dtype)
        return carry

    lax.fori_loop(0, turned.shape[0] // LANES // 4, four, 0)


def call(body, units, core, pieces, rest, out_shape):
    n, (features, m) = len(pieces), pieces[0].shape
    return pl.pallas_call(
        functools.partial(body, n, units),
        out_shape=out_shape,
        in_specs=[pl.BlockSpec(memory_space=pltpu.SMEM)] + [WHOLE] * (n + len(rest)),
        out_specs=jax.tree.map(lambda _: WHOLE, out_shape),
        scratch_shapes=[pltpu.VMEM((features, n * m), bf16), pltpu.VMEM((units, n * m), bf16)],
        compiler_params=pltpu.CompilerParams(vmem_limit_bytes=18 << 20),
    )(core, *pieces, *rest)


def begin(units, core, pieces, weights):
    n, m = len(pieces), pieces[0].shape[1]
    return call(begin_body, units, core, pieces, [weights], jax.ShapeDtypeStruct((units, n * m), bf16))


def finish(units, core, pieces, weights, first, dtype):
    out_shape = [jax.ShapeDtypeStruct(p.shape, dtype) for p in pieces]
    return call(finish_body, units, core, pieces, [*weights, first], out_shape)


def close_body(own, first, second, out):
    out[...] = (own[...] + first[...].astype(f32) + second[...].astype(f32)).T.astype(bf16)


def close(own, first, second):
    return pl.pallas_call(
        close_body,
        out_shape=jax.ShapeDtypeStruct(own.shape[::-1], bf16),
        in_specs=[WHOLE] * 3,
        out_specs=WHOLE,
        compiler_params=SMALL,
        name="close",
    )(own, first, second)


def local(tokens, norm_gain, gate_weight, up_weight, down_weight):
    core = lax.axis_index("c").astype(jnp.int32)[None]
    normed = norm(tokens, norm_gain)

    own, mate = {0: normed}, {0: swap(normed)}
    for d in (1, 2, 3, 4):
        own[d] = onward(own[d - 1], 1)
        if d < 4:
            mate[d] = onward(mate[d - 1], 1)

    rows = from_four(pack(gate_weight.T, up_weight.T, down_weight), ROWS)
    here, top, bottom = spread(rows)
    before_top = along_column(top, 1)
    after_bottom = along_column(bottom, -1)
    before_bottom = along_column(bottom, 1)
    after_top = along_column(top, -1)
    far_top = along_column(before_top, 1)
    far_bottom = along_column(after_bottom, -1)
    blocks = here, before_top, before_bottom, after_top, after_bottom, far_top, far_bottom
    others = []
    for b in blocks:
        others.append(swap(b))
    row, column = lax.axis_index("y").astype(jnp.int32)[None], lax.axis_index("x").astype(jnp.int32)[None]
    first = core == 0
    shape = (4, *here.shape)

    def held(place, blocks):
        most = hold(place, PARTS[:5], blocks[:5], shape)
        return hold(place, PARTS[5:], blocks[5:], shape, most)

    columns = held(jnp.where(first, row, column), blocks)
    weights = columns, held(jnp.where(first, column, row), others)

    units = down_weight.shape[0]
    groups = [(own[4], mate[3]), (own[3], mate[2]), (own[2], mate[1]), (own[1],), (own[0],)]
    firsts = []
    for g in groups:
        firsts.append(begin(units, core, g, columns))
    shares = []
    for i, (g, f) in enumerate(zip(groups, firsts)):
        shares.append(finish(units, core, g, weights, f, f32 if i else bf16))
    (own4, mate3), (own3, mate2), (own2, mate1), (own1,), (own0,) = shares

    def send(x):
        return onward(x.astype(bf16), -1)

    got_own = send(own4)
    got_mate = send(mate3)
    got_own = send(got_own.astype(f32) + own3)
    got_mate = send(got_mate.astype(f32) + mate2)
    got_own = send(got_own.astype(f32) + own2)
    got_mate = send(got_mate.astype(f32) + mate1)
    got_own = send(got_own.astype(f32) + own1)
    return close(own0, got_own, swap(got_mate))


def solution(mesh):
    fine = Mesh(mesh.devices.reshape(Y, X, Z, 2), AXES)
    fs, tp = ("y", "x"), ("z", "c")

    return jax.shard_map(
        local,
        mesh=fine,
        in_specs=(P(fs + tp, None), P(), P(fs, tp), P(fs, tp), P(tp, fs)),
        out_specs=P(fs + tp, None),
        check_vma=False,
    )
```

```python
import functools

import jax
import jax.numpy as jnp
from jax import lax
from jax.experimental import pallas as pl
from jax.experimental.pallas import tpu as pltpu
from jax.sharding import Mesh, PartitionSpec as P


eps_floor = 0.05
X, Y, Z = 4, 4, 8
AXES = ("y", "x", "z", "c")
LANES = 128
f32, bf16 = jnp.float32, jnp.bfloat16


def place(y, x, z, c):
    return ((y * X + x) * Z + z) * 2 + c


ROWS = [[place(y, x, z, 0) for x in range(X)] for y in range(Y) for z in range(Z)]
ROWS += [[place(y, x, z, 1) for y in range(Y)] for x in range(X) for z in range(Z)]
WHOLE = pl.BlockSpec(memory_space=pltpu.VMEM)
FULL = pltpu.CompilerParams(vmem_limit_bytes=67_000_000)
SMALL = pltpu.CompilerParams(vmem_limit_bytes=12 << 20)


def onward(x, by):
    pairs = [(2 * z + c, 2 * ((z + (by if c == 0 else -by)) % Z) + c) for z in range(Z) for c in range(2)]
    return lax.ppermute(x, ("z", "c"), pairs)


def along_column(x, by):
    flat = lambda y, x, c: (y % Y * X + x % X) * 2 + c
    pairs = [(flat(j, i, 0), flat(j + by, i, 0)) for j in range(Y) for i in range(X)]
    pairs += [(flat(j, i, 1), flat(j, i + by, 1)) for j in range(Y) for i in range(X)]
    return lax.ppermute(x, ("y", "x", "c"), pairs)


def swap(x):
    return lax.ppermute(x, "c", [(0, 1), (1, 0)])


def from_four(copies, groups):
    return lax.all_to_all(copies, AXES, 0, 0, axis_index_groups=groups, tiled=True)


def open_body(tokens_in, gain_in, gate_in, upper_in, down_in, normed_out, out, tokens, gain, down, normed, packed, sems):
    units = gate_in.shape[0]
    ends = [(tokens_in, tokens), (gain_in, gain), (down_in, down), (gate_in, packed.at[:units])]
    ends.append((upper_in, packed.at[units : 2 * units]))
    into = [pltpu.make_async_copy(*e, sems.at[i]) for i, e in enumerate(ends)]
    for c in into:
        c.start()
    for c in into[:2]:
        c.wait()
    values = tokens[...].astype(f32)
    factor = lax.rsqrt(jnp.mean(values * values, axis=-1, keepdims=True) + eps_floor)
    normed[...] = (values * factor * gain[...]).T.astype(bf16)
    copies = [pltpu.make_async_copy(normed, normed_out, sems.at[5])]
    copies[0].start()
    for c in into[2:]:
        c.wait()
    for at in range(0, units, LANES):
        n = min(LANES, units - at)
        rows = slice(2 * units + at, 2 * units + at + LANES)
        packed[rows, :n] = down[at : at + n].T
        if n < LANES:
            packed[rows, n:] = jnp.zeros((LANES, LANES - n), bf16)
    for k in range(4):
        copies.append(pltpu.make_async_copy(packed, out.at[k], sems.at[6 + k]))
        copies[-1].start()
    for c in copies:
        c.wait()


def opening(tokens, gain, gate, upper, down):
    units, (n, features) = gate.shape[0], tokens.shape
    shape = (2 * units + pl.cdiv(units, LANES) * LANES, LANES)
    remote = pl.BlockSpec(memory_space=pltpu.HBM)
    return pl.pallas_call(
        open_body,
        out_shape=[jax.ShapeDtypeStruct((features, n), bf16), jax.ShapeDtypeStruct((4, *shape), bf16)],
        in_specs=[remote] * 5,
        out_specs=[remote] * 2,
        scratch_shapes=[
            pltpu.VMEM(tokens.shape, bf16),
            pltpu.VMEM((1, features), f32),
            pltpu.VMEM(down.shape, bf16),
            pltpu.VMEM((features, n), bf16),
            pltpu.VMEM(shape, bf16),
            pltpu.SemaphoreType.DMA((10,)),
        ],
        compiler_params=FULL,
        name="opening",
    )(tokens, gain[None], gate, upper, down)


def spread_body(blocks, whole, *halves):
    n = halves[0].shape[0]
    for i, out in enumerate(halves):
        for k in range(4):
            part = blocks[k, n * i : n * (i + 1)]
            out[:, LANES * k : LANES * (k + 1)] = part
            whole[n * i : n * (i + 1), LANES * k : LANES * (k + 1)] = part


def spread(blocks):
    return pl.pallas_call(
        spread_body,
        out_shape=[jax.ShapeDtypeStruct((blocks.shape[1] // n, 4 * LANES), bf16) for n in (1, 2, 2)],
        in_specs=[WHOLE],
        out_specs=[WHOLE] * 3,
        compiler_params=SMALL,
        name="spread",
    )(blocks)


PARTS = ((0, None), (3, 0), (3, 1), (1, 0), (1, 1), (2, 0), (2, 1))


def hold_body(parts, sides, *refs):
    n, places, refs = len(parts), refs[:sides], refs[sides:]
    outs, sems = refs[-1 - sides : -1], refs[-1]
    half, copies = outs[0].shape[1] // 2, []
    for s, out in enumerate(outs):
        for i, (by, h) in enumerate(parts):
            at = (places[s][0] + by) % 4
            end = out.at[at] if h is None else out.at[at, half * h : half * (h + 1)]
            copies.append(pltpu.make_async_copy(refs[n * s + i], end, sems.at[n * s + i]))
    for c in copies:
        c.start()
    for c in copies:
        c.wait()


def hold(places, parts, blocks, shape, so_far=None):
    n, sides = len(blocks), len(places)
    more = [] if so_far is None else [so_far]
    remote = pl.BlockSpec(memory_space=pltpu.HBM)
    return pl.pallas_call(
        functools.partial(hold_body, parts, sides),
        out_shape=[jax.ShapeDtypeStruct(shape, bf16)] * sides,
        in_specs=[pl.BlockSpec(memory_space=pltpu.SMEM)] * sides + [remote] * n + [WHOLE] * len(more),
        out_specs=[WHOLE] * sides,
        input_output_aliases={n + sides: 0} if more else {},
        scratch_shapes=[pltpu.SemaphoreType.DMA((n,))],
        compiler_params=SMALL,
        name="hold",
    )(*places, *blocks, *more)


def order(core, b, w):
    return jnp.where(core == w, b, (b % 4) * 4 + b // 4)


def half_hidden(core, w, units, pieces, weights, turned):
    m, depth = pieces[0].shape[1], weights.shape[2]
    for b in range(turned.shape[0] // LANES):
        at = pl.ds(pl.multiple_of(order(core, b, w) * LANES, LANES), LANES)
        for i, piece in enumerate(pieces):
            turned[LANES * b : LANES * (b + 1), m * i : m * (i + 1)] = piece[at, :]
    both = jnp.dot(weights[0, : 2 * units], turned[:depth], preferred_element_type=f32)
    for k in range(1, 4):
        both += jnp.dot(weights[k, : 2 * units], turned[depth * k : depth * (k + 1)], preferred_element_type=f32)
    gate, upper = both[:units], both[units:]
    return (gate / (1.0 + jnp.exp(-gate)) * upper).astype(bf16)


def begin_body(n, units, core_ref, *refs):
    pieces, weights, out, turned = refs[:n], refs[n], refs[n + 1], refs[n + 2]
    out[...] = half_hidden(core_ref[0], 0, units, pieces, weights, turned)


def finish_body(n, units, core_ref, *refs):
    pieces, weights, first = refs[:n], refs[n : n + 2], refs[n + 2]
    outs, turned, held = refs[n + 3 : 2 * n + 3], refs[2 * n + 3], refs[2 * n + 4]
    core, m = core_ref[0], pieces[0].shape[1]
    hidden = first, held
    held[...] = half_hidden(core, 1, units, pieces, weights[1], turned)

    def four(group, carry):
        for j in range(4):
            b = group * 4 + j
            part = 0.0
            for w in (0, 1):
                at = order(core, b, w)
                lanes = pl.ds(pl.multiple_of(at % 4 * LANES, LANES), LANES)
                tiles = [weights[w][at // 4, r : r + LANES, lanes] for r in range(2 * units, weights[w].shape[1], LANES)]
                part += jnp.dot(jnp.concatenate(tiles, axis=1)[:, :units], hidden[w][...], preferred_element_type=f32)
            rows = pl.ds(pl.multiple_of(b * LANES, LANES), LANES)
            for i in range(n):
                outs[i][rows, :] = part[:, m * i : m * (i + 1)].astype(outs[i].dtype)
        return carry

    lax.fori_loop(0, turned.shape[0] // LANES // 4, four, 0)


def call(body, units, core, pieces, rest, out_shape):
    n, (features, m) = len(pieces), pieces[0].shape
    return pl.pallas_call(
        functools.partial(body, n, units),
        out_shape=out_shape,
        in_specs=[pl.BlockSpec(memory_space=pltpu.SMEM)] + [WHOLE] * (n + len(rest)),
        out_specs=jax.tree.map(lambda _: WHOLE, out_shape),
        scratch_shapes=[pltpu.VMEM((features, n * m), bf16), pltpu.VMEM((units, n * m), bf16)],
        compiler_params=pltpu.CompilerParams(vmem_limit_bytes=18 << 20),
    )(core, *pieces, *rest)


def begin(units, core, pieces, weights):
    n, m = len(pieces), pieces[0].shape[1]
    return call(begin_body, units, core, pieces, [weights], jax.ShapeDtypeStruct((units, n * m), bf16))


def finish(units, core, pieces, weights, first, dtype):
    out_shape = [jax.ShapeDtypeStruct(p.shape, dtype) for p in pieces]
    return call(finish_body, units, core, pieces, [*weights, first], out_shape)


def close_body(own, first, second, out):
    out[...] = (own[...] + first[...].astype(f32) + second[...].astype(f32)).T.astype(bf16)


def close(own, first, second):
    return pl.pallas_call(
        close_body,
        out_shape=jax.ShapeDtypeStruct(own.shape[::-1], bf16),
        in_specs=[WHOLE] * 3,
        out_specs=WHOLE,
        compiler_params=SMALL,
        name="close",
    )(own, first, second)


def local(tokens, norm_gain, gate_weight, up_weight, down_weight):
    core = lax.axis_index("c").astype(jnp.int32)[None]
    normed, packed = opening(tokens, norm_gain, gate_weight.T, up_weight.T, down_weight)

    own, mate = {0: normed}, {0: swap(normed)}
    for d in (1, 2, 3, 4):
        own[d] = onward(own[d - 1], 1)
        if d < 4:
            mate[d] = onward(mate[d - 1], 1)

    rows = from_four(packed, ROWS)
    here, top, bottom = spread(rows)
    before_top = along_column(top, 1)
    after_bottom = along_column(bottom, -1)
    before_bottom = along_column(bottom, 1)
    after_top = along_column(top, -1)
    far_top = along_column(before_top, 1)
    far_bottom = along_column(after_bottom, -1)
    blocks = here, before_top, before_bottom, after_top, after_bottom, far_top, far_bottom
    others = []
    for b in blocks:
        others.append(swap(b))
    row, column = lax.axis_index("y").astype(jnp.int32)[None], lax.axis_index("x").astype(jnp.int32)[None]
    first = core == 0
    mine, other = jnp.where(first, row, column), jnp.where(first, column, row)
    shape = (4, *here.shape)
    columns, others_columns = hold([mine, other], PARTS[:5], [*blocks[:5], *others[:5]], shape)
    (columns,) = hold([mine], PARTS[5:], blocks[5:], shape, columns)
    (others_columns,) = hold([other], PARTS[5:], others[5:], shape, others_columns)
    weights = columns, others_columns

    units = down_weight.shape[0]
    groups = [(own[4], mate[3]), (own[3], mate[2]), (own[2], mate[1]), (own[1],), (own[0],)]
    firsts = []
    for g in groups:
        firsts.append(begin(units, core, g, columns))
    shares = []
    for i, (g, f) in enumerate(zip(groups, firsts)):
        shares.append(finish(units, core, g, weights, f, f32 if i else bf16))
    (own4, mate3), (own3, mate2), (own2, mate1), (own1,), (own0,) = shares

    def send(x):
        return onward(x.astype(bf16), -1)

    got_own = send(own4)
    got_mate = send(mate3)
    got_own = send(got_own.astype(f32) + own3)
    got_mate = send(got_mate.astype(f32) + mate2)
    got_own = send(got_own.astype(f32) + own2)
    got_mate = send(got_mate.astype(f32) + mate1)
    got_own = send(got_own.astype(f32) + own1)
    return close(own0, got_own, swap(got_mate))


def solution(mesh):
    fine = Mesh(mesh.devices.reshape(Y, X, Z, 2), AXES)
    fs, tp = ("y", "x"), ("z", "c")

    return jax.shard_map(
        local,
        mesh=fine,
        in_specs=(P(fs + tp, None), P(), P(fs, tp), P(fs, tp), P(tp, fs)),
        out_specs=P(fs + tp, None),
        check_vma=False,
    )
```

```python
import functools

import jax
import jax.numpy as jnp
from jax import lax
from jax.experimental import pallas as pl
from jax.experimental.pallas import tpu as pltpu
from jax.sharding import Mesh, PartitionSpec as P


eps_floor = 0.05
X, Y, Z = 4, 4, 8
AXES = ("y", "x", "z", "c")
LANES = 128
f32, bf16 = jnp.float32, jnp.bfloat16


def place(y, x, z, c):
    return ((y * X + x) * Z + z) * 2 + c


ROWS = [[place(y, x, z, 0) for x in range(X)] for y in range(Y) for z in range(Z)]
ROWS += [[place(y, x, z, 1) for y in range(Y)] for x in range(X) for z in range(Z)]
WHOLE = pl.BlockSpec(memory_space=pltpu.VMEM)
FULL = pltpu.CompilerParams(vmem_limit_bytes=67_000_000)
SMALL = pltpu.CompilerParams(vmem_limit_bytes=12 << 20)


def onward(x, by):
    pairs = [(2 * z + c, 2 * ((z + (by if c == 0 else -by)) % Z) + c) for z in range(Z) for c in range(2)]
    return lax.ppermute(x, ("z", "c"), pairs)


def along_column(x, by):
    flat = lambda y, x, c: (y % Y * X + x % X) * 2 + c
    pairs = [(flat(j, i, 0), flat(j + by, i, 0)) for j in range(Y) for i in range(X)]
    pairs += [(flat(j, i, 1), flat(j, i + by, 1)) for j in range(Y) for i in range(X)]
    return lax.ppermute(x, ("y", "x", "c"), pairs)


def swap(x):
    return lax.ppermute(x, "c", [(0, 1), (1, 0)])


def from_four(copies, groups):
    return lax.all_to_all(copies, AXES, 0, 0, axis_index_groups=groups, tiled=True)


def open_body(tokens_in, gain_in, gate_in, upper_in, down_in, normed_out, out, tokens, gain, down, normed, packed, sems):
    units = gate_in.shape[0]
    ends = [(tokens_in, tokens), (gain_in, gain), (down_in, down), (gate_in, packed.at[:units])]
    ends.append((upper_in, packed.at[units : 2 * units]))
    into = [pltpu.make_async_copy(*e, sems.at[i]) for i, e in enumerate(ends)]
    for c in into:
        c.start()
    for c in into[:2]:
        c.wait()
    values = tokens[...].astype(f32)
    factor = lax.rsqrt(jnp.mean(values * values, axis=-1, keepdims=True) + eps_floor)
    normed[...] = (values * factor * gain[...]).T.astype(bf16)
    copies = [pltpu.make_async_copy(normed, normed_out, sems.at[5])]
    copies[0].start()
    for c in into[2:]:
        c.wait()
    for at in range(0, units, LANES):
        n = min(LANES, units - at)
        rows = slice(2 * units + at, 2 * units + at + LANES)
        packed[rows, :n] = down[at : at + n].T
        if n < LANES:
            packed[rows, n:] = jnp.zeros((LANES, LANES - n), bf16)
    for k in range(4):
        copies.append(pltpu.make_async_copy(packed, out.at[k], sems.at[6 + k]))
        copies[-1].start()
    for c in copies:
        c.wait()


def opening(tokens, gain, gate, upper, down):
    units, (n, features) = gate.shape[0], tokens.shape
    shape = (2 * units + pl.cdiv(units, LANES) * LANES, LANES)
    remote = pl.BlockSpec(memory_space=pltpu.HBM)
    return pl.pallas_call(
        open_body,
        out_shape=[jax.ShapeDtypeStruct((features, n), bf16), jax.ShapeDtypeStruct((4, *shape), bf16)],
        in_specs=[remote] * 5,
        out_specs=[remote] * 2,
        scratch_shapes=[
            pltpu.VMEM(tokens.shape, bf16),
            pltpu.VMEM((1, features), f32),
            pltpu.VMEM(down.shape, bf16),
            pltpu.VMEM((features, n), bf16),
            pltpu.VMEM(shape, bf16),
            pltpu.SemaphoreType.DMA((10,)),
        ],
        compiler_params=FULL,
        name="opening",
    )(tokens, gain[None], gate, upper, down)


def spread_body(blocks, whole, *halves):
    n = halves[0].shape[0]
    for i, out in enumerate(halves):
        for k in range(4):
            part = blocks[k, n * i : n * (i + 1)]
            out[:, LANES * k : LANES * (k + 1)] = part
            whole[n * i : n * (i + 1), LANES * k : LANES * (k + 1)] = part


def spread(blocks):
    return pl.pallas_call(
        spread_body,
        out_shape=[jax.ShapeDtypeStruct((blocks.shape[1] // n, 4 * LANES), bf16) for n in (1, 2, 2)],
        in_specs=[WHOLE],
        out_specs=[WHOLE] * 3,
        compiler_params=SMALL,
        name="spread",
    )(blocks)


PARTS = ((0, None), (3, 0), (3, 1), (1, 0), (1, 1), (2, 0), (2, 1))


def hold_body(parts, place_ref, *refs):
    n = len(parts)
    blocks, out, sems = refs[:n], refs[-2], refs[-1]
    half, at = out.shape[1] // 2, place_ref[0]
    copies = []
    for i, (by, h) in enumerate(parts):
        end = out.at[(at + by) % 4] if h is None else out.at[(at + by) % 4, half * h : half * (h + 1)]
        copies.append(pltpu.make_async_copy(blocks[i], end, sems.at[i]))
    for c in copies:
        c.start()
    for c in copies:
        c.wait()


def hold(place, parts, blocks, shape, so_far=None):
    n = len(parts)
    more = [] if so_far is None else [so_far]
    return pl.pallas_call(
        functools.partial(hold_body, parts),
        out_shape=jax.ShapeDtypeStruct(shape, bf16),
        in_specs=[pl.BlockSpec(memory_space=pltpu.SMEM)] + [pl.BlockSpec(memory_space=pltpu.HBM)] * n + [WHOLE] * len(more),
        out_specs=WHOLE,
        input_output_aliases={n + 1: 0} if more else {},
        scratch_shapes=[pltpu.SemaphoreType.DMA((n,))],
        compiler_params=SMALL,
        name="hold",
    )(place, *blocks, *more)


def order(core, b, w):
    return jnp.where(core == w, b, (b % 4) * 4 + b // 4)


def half_hidden(core, w, units, pieces, weights, turned):
    m, depth = pieces[0].shape[1], weights.shape[2]
    for b in range(turned.shape[0] // LANES):
        at = pl.ds(pl.multiple_of(order(core, b, w) * LANES, LANES), LANES)
        for i, piece in enumerate(pieces):
            turned[LANES * b : LANES * (b + 1), m * i : m * (i + 1)] = piece[at, :]
    both = jnp.dot(weights[0, : 2 * units], turned[:depth], preferred_element_type=f32)
    for k in range(1, 4):
        both += jnp.dot(weights[k, : 2 * units], turned[depth * k : depth * (k + 1)], preferred_element_type=f32)
    gate, upper = both[:units], both[units:]
    return (gate / (1.0 + jnp.exp(-gate)) * upper).astype(bf16)


def begin_body(n, units, core_ref, *refs):
    pieces, weights, out, turned = refs[:n], refs[n], refs[n + 1], refs[n + 2]
    out[...] = half_hidden(core_ref[0], 0, units, pieces, weights, turned)


def finish_body(n, units, core_ref, *refs):
    pieces, weights, first = refs[:n], refs[n : n + 2], refs[n + 2]
    outs, turned, held = refs[n + 3 : 2 * n + 3], refs[2 * n + 3], refs[2 * n + 4]
    core, m = core_ref[0], pieces[0].shape[1]
    hidden = first, held
    held[...] = half_hidden(core, 1, units, pieces, weights[1], turned)

    def four(group, carry):
        for j in range(4):
            b = group * 4 + j
            part = 0.0
            for w in (0, 1):
                at = order(core, b, w)
                lanes = pl.ds(pl.multiple_of(at % 4 * LANES, LANES), LANES)
                tiles = [weights[w][at // 4, r : r + LANES, lanes] for r in range(2 * units, weights[w].shape[1], LANES)]
                part += jnp.dot(jnp.concatenate(tiles, axis=1)[:, :units], hidden[w][...], preferred_element_type=f32)
            rows = pl.ds(pl.multiple_of(b * LANES, LANES), LANES)
            for i in range(n):
                outs[i][rows, :] = part[:, m * i : m * (i + 1)].astype(outs[i].dtype)
        return carry

    lax.fori_loop(0, turned.shape[0] // LANES // 4, four, 0)


def call(body, units, core, pieces, rest, out_shape):
    n, (features, m) = len(pieces), pieces[0].shape
    return pl.pallas_call(
        functools.partial(body, n, units),
        out_shape=out_shape,
        in_specs=[pl.BlockSpec(memory_space=pltpu.SMEM)] + [WHOLE] * (n + len(rest)),
        out_specs=jax.tree.map(lambda _: WHOLE, out_shape),
        scratch_shapes=[pltpu.VMEM((features, n * m), bf16), pltpu.VMEM((units, n * m), bf16)],
        compiler_params=pltpu.CompilerParams(vmem_limit_bytes=18 << 20),
    )(core, *pieces, *rest)


def begin(units, core, pieces, weights):
    n, m = len(pieces), pieces[0].shape[1]
    return call(begin_body, units, core, pieces, [weights], jax.ShapeDtypeStruct((units, n * m), bf16))


def finish(units, core, pieces, weights, first, dtype):
    out_shape = [jax.ShapeDtypeStruct(p.shape, dtype) for p in pieces]
    return call(finish_body, units, core, pieces, [*weights, first], out_shape)


def close_body(own, first, second, out):
    out[...] = (own[...] + first[...].astype(f32) + second[...].astype(f32)).T.astype(bf16)


def close(own, first, second):
    return pl.pallas_call(
        close_body,
        out_shape=jax.ShapeDtypeStruct(own.shape[::-1], bf16),
        in_specs=[WHOLE] * 3,
        out_specs=WHOLE,
        compiler_params=SMALL,
        name="close",
    )(own, first, second)


def local(tokens, norm_gain, gate_weight, up_weight, down_weight):
    core = lax.axis_index("c").astype(jnp.int32)[None]
    normed, packed = opening(tokens, norm_gain, gate_weight.T, up_weight.T, down_weight)

    own, mate = {0: normed}, {0: swap(normed)}
    for d in (1, 2, 3, 4):
        own[d] = onward(own[d - 1], 1)
        if d < 4:
            mate[d] = onward(mate[d - 1], 1)

    rows = from_four(packed, ROWS)
    here, top, bottom = spread(rows)
    before_top = along_column(top, 1)
    after_bottom = along_column(bottom, -1)
    before_bottom = along_column(bottom, 1)
    after_top = along_column(top, -1)
    far_top = along_column(before_top, 1)
    far_bottom = along_column(after_bottom, -1)
    blocks = here, before_top, before_bottom, after_top, after_bottom, far_top, far_bottom
    others = []
    for b in blocks:
        others.append(swap(b))
    row, column = lax.axis_index("y").astype(jnp.int32)[None], lax.axis_index("x").astype(jnp.int32)[None]
    first = core == 0
    shape = (4, *here.shape)

    def held(place, blocks):
        most = hold(place, PARTS[:5], blocks[:5], shape)
        return hold(place, PARTS[5:], blocks[5:], shape, most)

    columns = held(jnp.where(first, row, column), blocks)
    weights = columns, held(jnp.where(first, column, row), others)

    units = down_weight.shape[0]
    groups = [(own[4], mate[3]), (own[3], mate[2]), (own[2], mate[1]), (own[1],), (own[0],)]
    firsts = []
    for g in groups:
        firsts.append(begin(units, core, g, columns))
    shares = []
    for i, (g, f) in enumerate(zip(groups, firsts)):
        shares.append(finish(units, core, g, weights, f, f32 if i else bf16))
    (own4, mate3), (own3, mate2), (own2, mate1), (own1,), (own0,) = shares

    def send(x):
        return onward(x.astype(bf16), -1)

    got_own = send(own4)
    got_mate = send(mate3)
    got_own = send(got_own.astype(f32) + own3)
    got_mate = send(got_mate.astype(f32) + mate2)
    got_own = send(got_own.astype(f32) + own2)
    got_mate = send(got_mate.astype(f32) + mate1)
    got_own = send(got_own.astype(f32) + own1)
    return close(own0, got_own, swap(got_mate))


def solution(mesh):
    fine = Mesh(mesh.devices.reshape(Y, X, Z, 2), AXES)
    fs, tp = ("y", "x"), ("z", "c")

    return jax.shard_map(
        local,
        mesh=fine,
        in_specs=(P(fs + tp, None), P(), P(fs, tp), P(fs, tp), P(tp, fs)),
        out_specs=P(fs + tp, None),
        check_vma=False,
    )
```

```python
import functools

import jax
import jax.numpy as jnp
from jax import lax
from jax.experimental import pallas as pl
from jax.experimental.pallas import tpu as pltpu
from jax.sharding import Mesh, PartitionSpec as P


eps_floor = 0.05
X, Y, Z = 4, 4, 8
AXES = ("y", "x", "z", "c")
LANES = 128
f32, bf16 = jnp.float32, jnp.bfloat16


def place(y, x, z, c):
    return ((y * X + x) * Z + z) * 2 + c


ROWS = [[place(y, x, z, 0) for x in range(X)] for y in range(Y) for z in range(Z)]
ROWS += [[place(y, x, z, 1) for y in range(Y)] for x in range(X) for z in range(Z)]
WHOLE = pl.BlockSpec(memory_space=pltpu.VMEM)
FULL = pltpu.CompilerParams(vmem_limit_bytes=67_000_000)
SMALL = pltpu.CompilerParams(vmem_limit_bytes=12 << 20)


def onward(x, by):
    pairs = [(2 * z + c, 2 * ((z + (by if c == 0 else -by)) % Z) + c) for z in range(Z) for c in range(2)]
    return lax.ppermute(x, ("z", "c"), pairs)


def along_column(x, by):
    flat = lambda y, x, c: (y % Y * X + x % X) * 2 + c
    pairs = [(flat(j, i, 0), flat(j + by, i, 0)) for j in range(Y) for i in range(X)]
    pairs += [(flat(j, i, 1), flat(j, i + by, 1)) for j in range(Y) for i in range(X)]
    return lax.ppermute(x, ("y", "x", "c"), pairs)


def swap(x):
    return lax.ppermute(x, "c", [(0, 1), (1, 0)])


def from_four(copies, groups):
    return lax.all_to_all(copies, AXES, 0, 0, axis_index_groups=groups, tiled=True)


def open_body(tokens_in, gain_in, gate_in, upper_in, down_in, normed_out, out, tokens, gain, down, normed, packed, sems):
    units = gate_in.shape[0]
    ends = [(tokens_in, tokens), (gain_in, gain), (down_in, down), (gate_in, packed.at[:units])]
    ends.append((upper_in, packed.at[units : 2 * units]))
    into = [pltpu.make_async_copy(*e, sems.at[i]) for i, e in enumerate(ends)]
    for c in into:
        c.start()
    for c in into[:2]:
        c.wait()
    values = tokens[...].astype(f32)
    factor = lax.rsqrt(jnp.mean(values * values, axis=-1, keepdims=True) + eps_floor)
    normed[...] = (values * factor * gain[...]).T.astype(bf16)
    copies = [pltpu.make_async_copy(normed, normed_out, sems.at[5])]
    copies[0].start()
    for c in into[2:]:
        c.wait()
    for at in range(0, units, LANES):
        n = min(LANES, units - at)
        rows = slice(2 * units + at, 2 * units + at + LANES)
        packed[rows, :n] = down[at : at + n].T
        if n < LANES:
            packed[rows, n:] = jnp.zeros((LANES, LANES - n), bf16)
    for k in range(4):
        copies.append(pltpu.make_async_copy(packed, out.at[k], sems.at[6 + k]))
        copies[-1].start()
    for c in copies:
        c.wait()


def opening(tokens, gain, gate, upper, down):
    units, (n, features) = gate.shape[0], tokens.shape
    shape = (2 * units + pl.cdiv(units, LANES) * LANES, LANES)
    remote = pl.BlockSpec(memory_space=pltpu.HBM)
    return pl.pallas_call(
        open_body,
        out_shape=[jax.ShapeDtypeStruct((features, n), bf16), jax.ShapeDtypeStruct((4, *shape), bf16)],
        in_specs=[remote] * 5,
        out_specs=[remote] * 2,
        scratch_shapes=[
            pltpu.VMEM(tokens.shape, bf16),
            pltpu.VMEM((1, features), f32),
            pltpu.VMEM(down.shape, bf16),
            pltpu.VMEM((features, n), bf16),
            pltpu.VMEM(shape, bf16),
            pltpu.SemaphoreType.DMA((10,)),
        ],
        compiler_params=FULL,
        name="opening",
    )(tokens, gain[None], gate, upper, down)


def spread_body(blocks, whole, *halves):
    n = halves[0].shape[0]
    for i, out in enumerate(halves):
        for k in range(4):
            part = blocks[k, n * i : n * (i + 1)]
            out[:, LANES * k : LANES * (k + 1)] = part
            whole[n * i : n * (i + 1), LANES * k : LANES * (k + 1)] = part


def spread(blocks):
    return pl.pallas_call(
        spread_body,
        out_shape=[jax.ShapeDtypeStruct((blocks.shape[1] // n, 4 * LANES), bf16) for n in (1, 2, 2)],
        in_specs=[WHOLE],
        out_specs=[WHOLE] * 3,
        compiler_params=SMALL,
        name="spread",
    )(blocks)


PARTS = ((0, None), (3, 0), (3, 1), (1, 0), (1, 1), (2, 0), (2, 1))


def hold_body(parts, place_ref, *refs):
    n = len(parts)
    blocks, out, sems = refs[:n], refs[-2], refs[-1]
    half, at = out.shape[1] // 2, place_ref[0]
    copies = []
    for i, (by, h) in enumerate(parts):
        end = out.at[(at + by) % 4] if h is None else out.at[(at + by) % 4, half * h : half * (h + 1)]
        copies.append(pltpu.make_async_copy(blocks[i], end, sems.at[i]))
    for c in copies:
        c.start()
    for c in copies:
        c.wait()


def hold(place, parts, blocks, shape, so_far=None):
    n = len(parts)
    more = [] if so_far is None else [so_far]
    return pl.pallas_call(
        functools.partial(hold_body, parts),
        out_shape=jax.ShapeDtypeStruct(shape, bf16),
        in_specs=[pl.BlockSpec(memory_space=pltpu.SMEM)] + [pl.BlockSpec(memory_space=pltpu.HBM)] * n + [WHOLE] * len(more),
        out_specs=WHOLE,
        input_output_aliases={n + 1: 0} if more else {},
        scratch_shapes=[pltpu.SemaphoreType.DMA((n,))],
        compiler_params=SMALL,
        name="hold",
    )(place, *blocks, *more)


def order(core, b, w):
    return jnp.where(core == w, b, (b % 4) * 4 + b // 4)


def half_hidden(core, w, units, pieces, weights, turned):
    m, depth = pieces[0].shape[1], weights.shape[2]
    for b in range(turned.shape[0] // LANES):
        at = pl.ds(pl.multiple_of(order(core, b, w) * LANES, LANES), LANES)
        for i, piece in enumerate(pieces):
            turned[LANES * b : LANES * (b + 1), m * i : m * (i + 1)] = piece[at, :]
    both = jnp.dot(weights[0, : 2 * units], turned[:depth], preferred_element_type=f32)
    for k in range(1, 4):
        both += jnp.dot(weights[k, : 2 * units], turned[depth * k : depth * (k + 1)], preferred_element_type=f32)
    gate, upper = both[:units], both[units:]
    return (gate / (1.0 + jnp.exp(-gate)) * upper).astype(bf16)


def begin_body(n, units, core_ref, *refs):
    pieces, weights, out, turned = refs[:n], refs[n], refs[n + 1], refs[n + 2]
    out[...] = half_hidden(core_ref[0], 0, units, pieces, weights, turned)


def begin_far_body(n, units, core_ref, place_ref, *refs):
    pieces, (top, bottom, _, out, weights, turned, sems) = refs[:n], refs[n:]
    core, place, m, depth, half = core_ref[0], place_ref[0], pieces[0].shape[1], weights.shape[2], top.shape[0]
    far = (place + 2) % 4
    copies = [
        pltpu.make_async_copy(top, weights.at[far, :half], sems.at[0]),
        pltpu.make_async_copy(bottom, weights.at[far, half:], sems.at[1]),
    ]
    for c in copies:
        c.start()
    for b in range(turned.shape[0] // LANES):
        at = pl.ds(pl.multiple_of(order(core, b, 0) * LANES, LANES), LANES)
        for i, piece in enumerate(pieces):
            turned[LANES * b : LANES * (b + 1), m * i : m * (i + 1)] = piece[at, :]
    both = 0.0
    for by in (3, 0, 1, 2):
        if by == 2:
            for c in copies:
                c.wait()
        k = (place + by) % 4
        rows = turned[pl.ds(pl.multiple_of(k * depth, depth), depth), :]
        both += jnp.dot(weights[k, : 2 * units], rows, preferred_element_type=f32)
    gate, upper = both[:units], both[units:]
    out[...] = (gate / (1.0 + jnp.exp(-gate)) * upper).astype(bf16)


def begin_far(units, core, place, pieces, top, bottom, weights):
    n, (features, m) = len(pieces), pieces[0].shape
    smem, remote = pl.BlockSpec(memory_space=pltpu.SMEM), pl.BlockSpec(memory_space=pltpu.HBM)
    return pl.pallas_call(
        functools.partial(begin_far_body, n, units),
        out_shape=[jax.ShapeDtypeStruct((units, n * m), bf16), jax.ShapeDtypeStruct(weights.shape, bf16)],
        in_specs=[smem] * 2 + [WHOLE] * n + [remote] * 2 + [WHOLE],
        out_specs=[WHOLE] * 2,
        input_output_aliases={n + 4: 1},
        scratch_shapes=[pltpu.VMEM((features, n * m), bf16), pltpu.SemaphoreType.DMA((2,))],
        compiler_params=pltpu.CompilerParams(vmem_limit_bytes=18 << 20),
        name="begin_far",
    )(core, place, *pieces, top, bottom, weights)


def finish_body(n, units, core_ref, *refs):
    pieces, weights, first = refs[:n], refs[n : n + 2], refs[n + 2]
    outs, turned, held = refs[n + 3 : 2 * n + 3], refs[2 * n + 3], refs[2 * n + 4]
    core, m = core_ref[0], pieces[0].shape[1]
    hidden = first, held
    held[...] = half_hidden(core, 1, units, pieces, weights[1], turned)

    def four(group, carry):
        for j in range(4):
            b = group * 4 + j
            part = 0.0
            for w in (0, 1):
                at = order(core, b, w)
                lanes = pl.ds(pl.multiple_of(at % 4 * LANES, LANES), LANES)
                tiles = [weights[w][at // 4, r : r + LANES, lanes] for r in range(2 * units, weights[w].shape[1], LANES)]
                part += jnp.dot(jnp.concatenate(tiles, axis=1)[:, :units], hidden[w][...], preferred_element_type=f32)
            rows = pl.ds(pl.multiple_of(b * LANES, LANES), LANES)
            for i in range(n):
                outs[i][rows, :] = part[:, m * i : m * (i + 1)].astype(outs[i].dtype)
        return carry

    lax.fori_loop(0, turned.shape[0] // LANES // 4, four, 0)


def call(body, units, core, pieces, rest, out_shape):
    n, (features, m) = len(pieces), pieces[0].shape
    return pl.pallas_call(
        functools.partial(body, n, units),
        out_shape=out_shape,
        in_specs=[pl.BlockSpec(memory_space=pltpu.SMEM)] + [WHOLE] * (n + len(rest)),
        out_specs=jax.tree.map(lambda _: WHOLE, out_shape),
        scratch_shapes=[pltpu.VMEM((features, n * m), bf16), pltpu.VMEM((units, n * m), bf16)],
        compiler_params=pltpu.CompilerParams(vmem_limit_bytes=18 << 20),
    )(core, *pieces, *rest)


def begin(units, core, pieces, weights):
    n, m = len(pieces), pieces[0].shape[1]
    return call(begin_body, units, core, pieces, [weights], jax.ShapeDtypeStruct((units, n * m), bf16))


def finish(units, core, pieces, weights, first, dtype):
    out_shape = [jax.ShapeDtypeStruct(p.shape, dtype) for p in pieces]
    return call(finish_body, units, core, pieces, [*weights, first], out_shape)


def close_body(own, first, second, out):
    out[...] = (own[...] + first[...].astype(f32) + second[...].astype(f32)).T.astype(bf16)


def close(own, first, second):
    return pl.pallas_call(
        close_body,
        out_shape=jax.ShapeDtypeStruct(own.shape[::-1], bf16),
        in_specs=[WHOLE] * 3,
        out_specs=WHOLE,
        compiler_params=SMALL,
        name="close",
    )(own, first, second)


def local(tokens, norm_gain, gate_weight, up_weight, down_weight):
    core = lax.axis_index("c").astype(jnp.int32)[None]
    normed, packed = opening(tokens, norm_gain, gate_weight.T, up_weight.T, down_weight)

    own, mate = {0: normed}, {0: swap(normed)}
    for d in (1, 2, 3, 4):
        own[d] = onward(own[d - 1], 1)
        if d < 4:
            mate[d] = onward(mate[d - 1], 1)

    rows = from_four(packed, ROWS)
    here, top, bottom = spread(rows)
    before_top = along_column(top, 1)
    after_bottom = along_column(bottom, -1)
    before_bottom = along_column(bottom, 1)
    after_top = along_column(top, -1)
    far_top = along_column(before_top, 1)
    far_bottom = along_column(after_bottom, -1)
    blocks = here, before_top, before_bottom, after_top, after_bottom, far_top, far_bottom
    others = []
    for b in blocks:
        others.append(swap(b))
    row, column = lax.axis_index("y").astype(jnp.int32)[None], lax.axis_index("x").astype(jnp.int32)[None]
    first = core == 0
    shape = (4, *here.shape)

    def hold_most(place, blocks):
        return hold(place, PARTS[:5], blocks[:5], shape)

    units = down_weight.shape[0]
    groups = [(own[4], mate[3]), (own[3], mate[2]), (own[2], mate[1]), (own[1],), (own[0],)]
    mine, other = jnp.where(first, row, column), jnp.where(first, column, row)
    columns = hold_most(mine, blocks)
    start, columns = begin_far(units, core, mine, groups[0], *blocks[5:], columns)
    others_columns = hold_most(other, others)
    others_columns = hold(other, PARTS[5:], others[5:], shape, others_columns)
    weights = columns, others_columns

    firsts = [start]
    for i, g in enumerate(groups[1:], 1):
        firsts.append(begin(units, core, g, columns))
    shares = []
    for i, (g, f) in enumerate(zip(groups, firsts)):
        shares.append(finish(units, core, g, weights, f, f32 if i else bf16))
    (own4, mate3), (own3, mate2), (own2, mate1), (own1,), (own0,) = shares

    def send(x):
        return onward(x.astype(bf16), -1)

    got_own = send(own4)
    got_mate = send(mate3)
    got_own = send(got_own.astype(f32) + own3)
    got_mate = send(got_mate.astype(f32) + mate2)
    got_own = send(got_own.astype(f32) + own2)
    got_mate = send(got_mate.astype(f32) + mate1)
    got_own = send(got_own.astype(f32) + own1)
    got_mate = swap(got_mate)
    return close(own0, got_own, got_mate)


def solution(mesh):
    fine = Mesh(mesh.devices.reshape(Y, X, Z, 2), AXES)
    fs, tp = ("y", "x"), ("z", "c")

    return jax.shard_map(
        local,
        mesh=fine,
        in_specs=(P(fs + tp, None), P(), P(fs, tp), P(fs, tp), P(tp, fs)),
        out_specs=P(fs + tp, None),
        check_vma=False,
    )
```
